32 devices in a mesh: sp: 8 (over z, x), tp: 4 (over y, core).
Axes of the slice: x: 2, y: 2, z: 4, core: 2. Of those that a mesh axis runs over, the one named last changes fastest.
Arguments:
- layer_input: bfloat16 [8, 4096, 2048], P(None, ('sp', 'tp')), may hold values from -6 to 6
- norm_gain: bfloat16 [2048], replicated, may hold values from 0.099609375 to 1.8984375
- key_weight: bfloat16 [2048, 1024], replicated, may hold values from -0.125 to 0.125
- value_weight: bfloat16 [2048, 1024], replicated, may hold values from -0.125 to 0.125
- new_query: bfloat16 [8, 1024], P('sp', 'tp'), may hold values from -12 to 12
- score_offset: float32 [8], replicated, may hold values from -10 to -3.5
Outputs:
- key_cache: bfloat16 [8, 4096, 1024], P('sp', None, 'tp')
- value_cache: bfloat16 [8, 4096, 1024], P('sp', None, 'tp')
- first_read: float32 [8, 1024], P('sp', 'tp')
The draws below stay inside these ranges and needn't reach their ends.
All inputs are finite; a program needn't handle non-finite values.
Results may differ from the reference program's by a relative error of at most 0.0082.
Values may be sent and summed in bfloat16 or wider, within the bound.
A program may use at most 128 MiB of HBM per device.

```python
import jax
import jax.numpy as jnp
from jax import lax

D = 2048
HEADS = 8
HEAD_DIM = 128
SEQS = 8
LENGTH = 4096


def draw_score_offset(key, part):
    return jax.random.uniform(key, (HEADS,), jnp.float32, -10.0, -3.5)


def steps_of(own_key, extent, cuts, least, top_value):
    def one(position, shards_of):
        heights = jax.random.uniform(jax.random.fold_in(jax.random.fold_in(own_key, 6), position), (shards_of,), jnp.float32, least / len(cuts), top_value / len(cuts))
        return jnp.repeat(jnp.exp(heights), extent[position] // shards_of).reshape((-1,) + (1,) * (len(extent) - position - 1))

    factor_of = one(*cuts[0])
    for cut in cuts[1:]:
        factor_of = factor_of * one(*cut)
    return factor_of


def gaussian(own_key, shape, scale, most, pieces=(), kind=jnp.bfloat16):
    array = jax.random.normal(own_key, shape, jnp.float32) * scale
    if len(pieces) > 0:
        array = steps_of(own_key, shape, pieces, -0.22, 0.18) * array
    return jnp.clip(array, min=-most, max=most).astype(kind)


def setup_inputs(seed: int = 0) -> dict:
    arg_keys = jax.random.split(jax.random.key(seed), 7)
    layer_input = gaussian(arg_keys[0], (SEQS, LENGTH, D), 1.0, 6.0, ((1, 32),))
    norm_gain = jnp.clip(1.0 + 0.18 * jax.random.normal(arg_keys[1], (D,), jnp.float32), 0.099609375, 1.8984375).astype(jnp.bfloat16)
    key_weight = gaussian(arg_keys[2], (D, HEADS * HEAD_DIM), D ** -0.5, 0.125)
    value_weight = gaussian(arg_keys[3], (D, HEADS * HEAD_DIM), D ** -0.5, 0.125)
    new_query = gaussian(arg_keys[4], (SEQS, HEADS * HEAD_DIM), 2.0, 12.0, ((0, 8), (1, 4)))
    score_offset = draw_score_offset(jax.random.fold_in(arg_keys[6], 71), 0)
    return {"layer_input": layer_input, "norm_gain": norm_gain, "key_weight": key_weight, "value_weight": value_weight, "new_query": new_query, "score_offset": score_offset}


norm_epsilon = 1e-06

def reference(layer_input, norm_gain, key_weight, value_weight, new_query, score_offset):

    def project(rows):
        wide = rows.astype(jnp.float32)
        normed = (wide * lax.rsqrt(lax.optimization_barrier(jnp.mean(wide * wide, axis=-1, keepdims=True)) + norm_epsilon) * norm_gain.astype(jnp.float32)).astype(jnp.bfloat16)
        keys = jnp.dot(normed, key_weight, preferred_element_type=jnp.float32).astype(jnp.bfloat16)
        values = jnp.dot(normed, value_weight, preferred_element_type=jnp.float32).astype(jnp.bfloat16)
        return (keys, values)
    key_cache, value_cache = lax.map(project, layer_input)
    query_heads = new_query.reshape(SEQS, HEADS, HEAD_DIM).astype(jnp.float32)
    key_heads = key_cache.reshape(SEQS, LENGTH, HEADS, HEAD_DIM).astype(jnp.float32)
    value_heads = value_cache.reshape(SEQS, LENGTH, HEADS, HEAD_DIM).astype(jnp.float32)
    scores = jnp.einsum('shd,sphd->shp', query_heads, key_heads, precision=lax.Precision.HIGHEST)
    scores = scores * HEAD_DIM ** (-0.5) + score_offset[None, :, None]
    log_rest = jax.nn.log_sigmoid(-scores)
    later = lax.cumsum(log_rest, axis=2, reverse=True) - log_rest
    weights = jnp.exp(jax.nn.log_sigmoid(scores) + later).astype(jnp.bfloat16)
    reading = jnp.einsum('shp,sphd->shd', weights.astype(jnp.float32), value_heads, precision=lax.Precision.HIGHEST)
    first_read = reading * lax.rsqrt(lax.optimization_barrier(jnp.mean(reading * reading, axis=-1, keepdims=True)) + norm_epsilon)
    return (key_cache, value_cache, first_read.reshape(SEQS, HEADS * HEAD_DIM))
```

```python
import functools

import jax
import jax.numpy as jnp
from jax import lax
from jax.experimental import pallas as pl
from jax.experimental.pallas import tpu as pltpu
from jax.sharding import PartitionSpec as P

norm_epsilon = 1e-06
MESH = pl.DeviceIdType.MESH
NORM_ROWS = 16
BATCH = 4
VMEM_BYTES = 64000000


class Layout:
    def __init__(self, seqs, groups):
        self.seqs = seqs
        self.groups = groups
        self.sides = 2 if seqs % 2 == 0 else 1
        self.cores = 2 if groups % 2 == 0 else 1
        self.planes = seqs // self.sides
        self.ranks = groups // self.cores
        self.per_plane = self.sides * groups
        seq = lax.axis_index("sp")
        group = lax.axis_index("tp")
        self.me = seq * groups + group
        self.seq = seq
        self.group = group
        self.side = lax.rem(seq, self.sides)
        self.plane = seq // self.sides
        self.core = lax.rem(group, self.cores)
        self.rank = group // self.cores
        self.upper = (2 * self.plane >= self.planes).astype(jnp.int32)

    def far_plane(self, step):
        return self.upper * step + (1 - self.upper) * (self.planes - 1 - step)

    def send_seq(self, half):
        side = lax.rem(self.side + half + self.core, self.sides)
        return self.far_plane(half // self.sides) * self.sides + side

    def send_group(self, turn):
        rank = lax.rem(self.rank + turn // self.cores, self.ranks)
        return rank * self.cores + lax.rem(self.core + turn, self.cores)

    def source_plane(self, step):
        near = self.planes - self.planes // 2
        plane = self.upper * (self.planes - 1 - self.plane) + (1 - self.upper) * self.plane
        first = lax.rem(plane + step, near)
        later = self.planes - 1 - (step - near)
        is_near = (step < near).astype(jnp.int32)
        plane = is_near * first + (1 - is_near) * later
        return self.upper * (self.planes - 1 - plane) + (1 - self.upper) * plane

    def source(self, index):
        within = lax.rem(index, self.per_plane)
        turn = lax.rem(within, self.groups)
        core = lax.rem(self.core + self.cores - lax.rem(turn, self.cores), self.cores)
        flip = lax.rem(within // self.groups + core, self.sides)
        side = lax.rem(self.side + self.sides - flip, self.sides)
        rank = lax.rem(self.rank + self.ranks - turn // self.cores, self.ranks)
        plane = self.source_plane(index // self.per_plane)
        return (plane * self.sides + side) * self.groups + rank * self.cores + core


def read_block(query, offsets, earlier, keys, values, head_dim):
    scores = lax.dot_general(
        query, keys, (((1,), (1,)), ((), ())), preferred_element_type=jnp.float32
    )
    scores = scores * head_dim ** (-0.5) + offsets
    soft = jnp.log1p(jnp.exp(-jnp.abs(scores)))
    rest = -jnp.maximum(scores, 0.0) - soft
    positions = scores.shape[1]
    sums = jnp.zeros((scores.shape[0], 2 * positions), jnp.float32)
    left = rest
    for _ in range(3):
        piece = left.astype(jnp.bfloat16)
        left = left - piece.astype(jnp.float32)
        sums = sums + jnp.dot(piece, earlier, preferred_element_type=jnp.float32)
    later = sums[:, :positions]
    weights = jnp.exp(jnp.minimum(scores, 0.0) - soft + later).astype(jnp.bfloat16)
    reading = jnp.dot(weights, values, preferred_element_type=jnp.float32)
    return reading, sums[:, positions:]


def later_matrix(positions):
    row = lax.broadcasted_iota(jnp.int32, (positions, 2 * positions), 0)
    col = lax.broadcasted_iota(jnp.int32, (positions, 2 * positions), 1)
    return ((row > col) | (col >= positions)).astype(jnp.float32).astype(jnp.bfloat16)


def exchange_kernel(
    seqs,
    groups,
    local_heads,
    x_hbm,
    gain_hbm,
    key_w_hbm,
    value_w_hbm,
    query_hbm,
    offset_hbm,
    arrived,
    block_read,
    block_rest,
    masked_query,
    offsets,
    x_buf,
    gain,
    query,
    offset,
    normed,
    key_w,
    value_w,
    outgoing,
    x_sem,
    w_sem,
    small_sem,
    send_sem,
    recv_sem,
):
    positions = x_buf.shape[1]
    width = x_buf.shape[2]
    columns = query.shape[1]
    head_dim = columns // local_heads
    pad = masked_query.shape[0]
    devices = seqs * groups
    at = Layout(seqs, groups)
    me = at.me

    def x_copy(half):
        return pltpu.make_async_copy(x_hbm.at[at.send_seq(half)], x_buf.at[half], x_sem.at[half])

    def w_copy(turn, part):
        group = at.send_group(turn)
        cols = pl.ds(pl.multiple_of(group * columns, columns), columns)
        source = (key_w_hbm, value_w_hbm)[part].at[:, cols]
        return pltpu.make_async_copy(source, (key_w, value_w)[part].at[turn], w_sem.at[part, turn])

    small_copies = (
        pltpu.make_async_copy(gain_hbm, gain, small_sem.at[0]),
        pltpu.make_async_copy(query_hbm, query, small_sem.at[1]),
        pltpu.make_async_copy(offset_hbm, offset, small_sem.at[2]),
    )

    barrier = pltpu.get_barrier_semaphore()

    @pl.loop(0, devices)
    def _(device):
        @pl.when(device != me)
        def _():
            pl.semaphore_signal(
                barrier,
                inc=1,
                device_id=(device // groups, lax.rem(device, groups)),
                device_id_type=MESH,
            )

    x_copy(0).start()
    for copy in small_copies:
        copy.start()
    for turn in range(groups):
        w_copy(turn, 0).start()
        w_copy(turn, 1).start()
        if turn == 0 and seqs > 1:
            x_copy(1).start()

    @pl.loop(2, seqs)
    def _(half):
        x_copy(half).start()

    def block_rows(device):
        return pl.ds(pl.multiple_of(device * positions, positions), positions)

    def remote(half, turn, part):
        seq = at.send_seq(half)
        group = at.send_group(turn)
        device = seq * groups + group
        cols = pl.ds(part * columns, columns)
        return device, pltpu.make_async_remote_copy(
            src_ref=outgoing.at[half, turn, :, cols],
            dst_ref=arrived.at[block_rows(me), cols],
            send_sem=send_sem.at[device],
            recv_sem=recv_sem.at[me],
            device_id=(seq, group),
            device_id_type=MESH,
        )

    def launch(half, turn, part):
        device, copy = remote(half, turn, part)

        @pl.when(device != me)
        def _():
            copy.start()

        @pl.when(device == me)
        def _():
            cols = slice(part * columns, (part + 1) * columns)
            arrived[block_rows(me), cols] = outgoing[half, turn, :, cols]

    def norm(half):
        x_copy(half).wait()

        @pl.loop(0, positions // NORM_ROWS)
        def _(chunk):
            rows = pl.ds(pl.multiple_of(chunk * NORM_ROWS, NORM_ROWS), NORM_ROWS)
            wide = x_buf[half, rows, :].astype(jnp.float32)
            scale = lax.rsqrt(jnp.sum(wide * wide, axis=-1, keepdims=True) / width + norm_epsilon)
            normed[rows, :] = (wide * scale * gain[...].astype(jnp.float32).reshape(1, width)).astype(
                jnp.bfloat16
            )

    def project(half, turn, part):
        weight = (key_w, value_w)[part]
        outgoing[half, turn, :, part * columns : (part + 1) * columns] = jnp.dot(
            normed[...], weight[turn], preferred_element_type=jnp.float32
        ).astype(jnp.bfloat16)

    small_copies[0].wait()

    @pl.loop(0, devices)
    def _(index):
        half = index // groups
        turn = lax.rem(index, groups)

        @pl.when(turn == 0)
        def _():
            norm(half)

        @pl.when(half == 0)
        def _():
            w_copy(turn, 0).wait()

        project(half, turn, 0)

        @pl.when(index == 0)
        def _():
            pl.semaphore_wait(barrier, devices - 1)

        @pl.when(index > 0)
        def _():
            launch((index - 1) // groups, lax.rem(index - 1, groups), 1)

        @pl.when(half == 0)
        def _():
            w_copy(turn, 1).wait()

        project(half, turn, 1)
        launch(half, turn, 0)

    small_copies[1].wait()
    small_copies[2].wait()
    row = lax.broadcasted_iota(jnp.int32, (pad, columns), 0)
    col = lax.broadcasted_iota(jnp.int32, (pad, columns), 1)
    masked_query[...] = jnp.where(
        row == col // head_dim,
        jnp.broadcast_to(query[...].astype(jnp.float32), (pad, columns)),
        0.0,
    ).astype(jnp.bfloat16)
    score_row = lax.broadcasted_iota(jnp.int32, (pad, positions), 0)
    head_offsets = jnp.zeros((pad, positions), jnp.float32)
    for head in range(local_heads):
        head_offsets = jnp.where(
            score_row == head, offset[at.group * local_heads + head], head_offsets
        )
    offsets[...] = head_offsets
    launch(seqs - 1, groups - 1, 1)

    earlier = later_matrix(positions)

    def wait_block(source):
        @pl.when(source != me)
        def _():
            pltpu.make_async_copy(
                outgoing.at[0, 0], arrived.at[block_rows(source)], recv_sem.at[source]
            ).wait()

    @pl.loop(0, devices // BATCH)
    def _(batch):
        sources = [at.source(batch * BATCH + k) for k in range(BATCH)]
        for source in sources:
            wait_block(source)

        @pl.when(batch < devices // BATCH - 1)
        def _():
            for source in sources:
                rows = block_rows(source)
                reading, rest = read_block(
                    masked_query[...],
                    offsets[...],
                    earlier,
                    arrived[rows, :columns],
                    arrived[rows, columns:],
                    head_dim,
                )
                block_read[source] = reading
                block_rest[source] = rest

    @pl.loop(0, devices)
    def _(index):
        half = index // groups
        turn = lax.rem(index, groups)
        device = at.send_seq(half) * groups + at.send_group(turn)

        @pl.when(device != me)
        def _():
            pltpu.make_async_copy(
                outgoing.at[half, turn], arrived.at[block_rows(device)], send_sem.at[device]
            ).wait()


def finish_kernel(
    seqs,
    groups,
    local_heads,
    arrived,
    block_read,
    block_rest,
    masked_query,
    offsets,
    keys_hbm,
    values_hbm,
    read_hbm,
    last_read,
    last_rest,
    read,
    out_sem,
    read_sem,
):
    devices = seqs * groups
    length = arrived.shape[0]
    positions = length // devices
    columns = masked_query.shape[1]
    head_dim = columns // local_heads
    at = Layout(seqs, groups)
    pieces = out_sem.shape[1]
    span = length // pieces

    def out_copies(piece):
        rows = pl.ds(piece * span, span)
        return (
            pltpu.make_async_copy(
                arrived.at[rows, pl.ds(0, columns)], keys_hbm.at[rows], out_sem.at[0, piece]
            ),
            pltpu.make_async_copy(
                arrived.at[rows, pl.ds(columns, columns)], values_hbm.at[rows], out_sem.at[1, piece]
            ),
        )

    for piece in range(pieces):
        for copy in out_copies(piece):
            copy.start()

    sources = [at.source(jnp.int32(devices - BATCH + k)) for k in range(BATCH)]
    earlier = later_matrix(positions)
    last_read[...] = block_read[...]
    last_rest[...] = block_rest[...]
    for source in sources:
        rows = pl.ds(pl.multiple_of(source * positions, positions), positions)
        reading, rest = read_block(
            masked_query[...],
            offsets[...],
            earlier,
            arrived[rows, :columns],
            arrived[rows, columns:],
            head_dim,
        )
        last_read[source] = reading
        last_rest[source] = rest

    reading = jnp.zeros(last_read.shape[1:], jnp.float32)
    after = jnp.zeros(last_rest.shape[1:], jnp.float32)
    for device in reversed(range(devices)):
        scale = jnp.exp(after)
        reading = reading + jnp.concatenate([scale] * (columns // positions), axis=1) * last_read[device]
        after = after + last_rest[device]
    for head in range(local_heads):
        own_cols = slice(head * head_dim, (head + 1) * head_dim)
        part = reading[head : head + 1, own_cols]
        read[:, own_cols] = part * lax.rsqrt(
            jnp.mean(part * part, axis=-1, keepdims=True) + norm_epsilon
        )
    read_copy = pltpu.make_async_copy(read, read_hbm, read_sem)
    read_copy.start()
    for piece in range(pieces):
        for copy in out_copies(piece):
            copy.wait()
    read_copy.wait()


def shards(seqs, groups, layer_input, norm_gain, key_weight, value_weight, new_query, score_offset):
    seq_count, positions, width = layer_input.shape
    columns = new_query.shape[1]
    local_heads = score_offset.shape[0] // groups
    pad = -(-local_heads // 8) * 8
    devices = seqs * groups
    length = devices * positions
    hbm = pl.BlockSpec(memory_space=pltpu.HBM)
    vmem = pl.BlockSpec(memory_space=pltpu.VMEM)
    passed_bytes = 4 * length * columns + 4 * devices * pad * (columns + positions)
    passed = pl.pallas_call(
        functools.partial(exchange_kernel, seqs, groups, local_heads),
        out_shape=(
            pltpu.VMEM((length, 2 * columns), jnp.bfloat16),
            pltpu.VMEM((devices, pad, columns), jnp.float32),
            pltpu.VMEM((devices, pad, positions), jnp.float32),
            pltpu.VMEM((pad, columns), jnp.bfloat16),
            pltpu.VMEM((pad, positions), jnp.float32),
        ),
        in_specs=[hbm] * 6,
        out_specs=(vmem,) * 5,
        scratch_shapes=[
            pltpu.VMEM((seq_count, positions, width), jnp.bfloat16),
            pltpu.VMEM((width,), jnp.bfloat16),
            pltpu.VMEM((1, columns), jnp.bfloat16),
            pltpu.SMEM(score_offset.shape, jnp.float32),
            pltpu.VMEM((positions, width), jnp.bfloat16),
            pltpu.VMEM((groups, width, columns), jnp.bfloat16),
            pltpu.VMEM((groups, width, columns), jnp.bfloat16),
            pltpu.VMEM((seqs, groups, positions, 2 * columns), jnp.bfloat16),
            pltpu.SemaphoreType.DMA((seq_count,)),
            pltpu.SemaphoreType.DMA((2, groups)),
            pltpu.SemaphoreType.DMA((3,)),
            pltpu.SemaphoreType.DMA((devices,)),
            pltpu.SemaphoreType.DMA((devices,)),
        ],
        compiler_params=pltpu.CompilerParams(
            collective_id=0, has_side_effects=True, vmem_limit_bytes=VMEM_BYTES - passed_bytes
        ),
    )(layer_input, norm_gain, key_weight, value_weight, new_query, score_offset)
    keys, values, read = pl.pallas_call(
        functools.partial(finish_kernel, seqs, groups, local_heads),
        out_shape=(
            jax.ShapeDtypeStruct((length, columns), jnp.bfloat16),
            jax.ShapeDtypeStruct((length, columns), jnp.bfloat16),
            jax.ShapeDtypeStruct((1, columns), jnp.float32),
        ),
        in_specs=[vmem] * 5,
        out_specs=(hbm,) * 3,
        scratch_shapes=[
            pltpu.VMEM((devices, pad, columns), jnp.float32),
            pltpu.VMEM((devices, pad, positions), jnp.float32),
            pltpu.VMEM((1, columns), jnp.float32),
            pltpu.SemaphoreType.DMA((2, 4)),
            pltpu.SemaphoreType.DMA,
        ],
        compiler_params=pltpu.CompilerParams(vmem_limit_bytes=20000000),
    )(*passed)
    return (keys[None], values[None], read)


def solution(mesh):
    seqs = mesh.shape["sp"]
    groups = mesh.shape["tp"]
    placed = (P(None, ("sp", "tp"), None), P(), P(), P(), P("sp", "tp"), P())
    return jax.shard_map(
        functools.partial(shards, seqs, groups),
        mesh=mesh,
        in_specs=placed,
        out_specs=(P("sp", None, "tp"), P("sp", None, "tp"), P("sp", "tp")),
        check_vma=False,
    )
```

```python
import functools

import jax
import jax.numpy as jnp
from jax import lax
from jax.experimental import pallas as pl
from jax.experimental.pallas import tpu as pltpu
from jax.sharding import PartitionSpec as P

norm_epsilon = 1e-06
MESH = pl.DeviceIdType.MESH
NORM_ROWS = 64
LANES = 128
BATCH = 4
EARLY = 2
VMEM_BYTES = 64000000


class Layout:
    def __init__(self, seqs, groups):
        self.seqs = seqs
        self.groups = groups
        self.sides = 2 if seqs % 2 == 0 else 1
        self.cores = 2 if groups % 2 == 0 else 1
        self.planes = seqs // self.sides
        self.ranks = groups // self.cores
        self.per_plane = self.sides * groups
        seq = lax.axis_index("sp")
        group = lax.axis_index("tp")
        self.me = seq * groups + group
        self.seq = seq
        self.group = group
        self.side = lax.rem(seq, self.sides)
        self.plane = seq // self.sides
        self.core = lax.rem(group, self.cores)
        self.rank = group // self.cores
        self.upper = (2 * self.plane >= self.planes).astype(jnp.int32)

    def far_plane(self, step):
        return self.upper * step + (1 - self.upper) * (self.planes - 1 - step)

    def send_seq(self, half):
        side = lax.rem(self.side + half + self.core, self.sides)
        return self.far_plane(half // self.sides) * self.sides + side

    def near_half(self):
        if self.planes == 1:
            return jnp.int32(0)
        step = self.upper * (self.plane - 1) + (1 - self.upper) * (self.planes - 2 - self.plane)
        return step * self.sides

    def place(self, index):
        first = self.near_half() * self.groups
        late = index - EARLY
        late = late + EARLY * (late >= first).astype(jnp.int32)
        number = jnp.where(index < EARLY, first + index, late)
        return number // self.groups, lax.rem(number, self.groups)

    def send_group(self, turn):
        rank = lax.rem(self.rank + turn // self.cores, self.ranks)
        return rank * self.cores + lax.rem(self.core + turn, self.cores)

    def source_plane(self, step):
        near = self.planes - self.planes // 2
        plane = self.upper * (self.planes - 1 - self.plane) + (1 - self.upper) * self.plane
        first = lax.rem(plane + step, near)
        later = self.planes - 1 - (step - near)
        is_near = (step < near).astype(jnp.int32)
        plane = is_near * first + (1 - is_near) * later
        return self.upper * (self.planes - 1 - plane) + (1 - self.upper) * plane

    def source(self, index):
        within = lax.rem(index, self.per_plane)
        turn = lax.rem(within, self.groups)
        core = lax.rem(self.core + self.cores - lax.rem(turn, self.cores), self.cores)
        flip = lax.rem(within // self.groups + core, self.sides)
        side = lax.rem(self.side + self.sides - flip, self.sides)
        rank = lax.rem(self.rank + self.ranks - turn // self.cores, self.ranks)
        plane = self.source_plane(index // self.per_plane)
        return (plane * self.sides + side) * self.groups + rank * self.cores + core


def read_block(query, offsets, earlier, keys, values, head_dim):
    scores = lax.dot_general(
        query, keys, (((1,), (1,)), ((), ())), preferred_element_type=jnp.float32
    )
    scores = scores * head_dim ** (-0.5) + offsets
    soft = jnp.log1p(jnp.exp(-jnp.abs(scores)))
    rest = -jnp.maximum(scores, 0.0) - soft
    positions = scores.shape[1]
    sums = jnp.zeros((scores.shape[0], 2 * positions), jnp.float32)
    left = rest
    for _ in range(3):
        piece = left.astype(jnp.bfloat16)
        left = left - piece.astype(jnp.float32)
        sums = sums + jnp.dot(piece, earlier, preferred_element_type=jnp.float32)
    later = sums[:, :positions]
    weights = jnp.exp(jnp.minimum(scores, 0.0) - soft + later).astype(jnp.bfloat16)
    reading = jnp.dot(weights, values, preferred_element_type=jnp.float32)
    return reading, sums[:, positions:]


def later_matrix(positions):
    row = lax.broadcasted_iota(jnp.int32, (positions, 2 * positions), 0)
    col = lax.broadcasted_iota(jnp.int32, (positions, 2 * positions), 1)
    return ((row > col) | (col >= positions)).astype(jnp.float32).astype(jnp.bfloat16)


def exchange_kernel(
    seqs,
    groups,
    local_heads,
    x_hbm,
    gain_hbm,
    key_w_hbm,
    value_w_hbm,
    query_hbm,
    offset_hbm,
    arrived,
    block_read,
    block_rest,
    masked_query,
    offsets,
    x_buf,
    gain,
    query,
    offset,
    normed,
    key_w,
    value_w,
    outgoing,
    x_sem,
    w_sem,
    small_sem,
    send_sem,
    recv_sem,
    round_sem,
):
    positions = x_buf.shape[1]
    width = x_buf.shape[2]
    columns = query.shape[1]
    head_dim = columns // local_heads
    pad = masked_query.shape[0]
    devices = seqs * groups
    at = Layout(seqs, groups)
    me = at.me

    def x_copy(half):
        return pltpu.make_async_copy(x_hbm.at[at.send_seq(half)], x_buf.at[half], x_sem.at[half])

    def w_copy(turn, part):
        group = at.send_group(turn)
        cols = pl.ds(pl.multiple_of(group * columns, columns), columns)
        source = (key_w_hbm, value_w_hbm)[part].at[:, cols]
        return pltpu.make_async_copy(source, (key_w, value_w)[part].at[turn], w_sem.at[part, turn])

    small_copies = (
        pltpu.make_async_copy(gain_hbm, gain, small_sem.at[0]),
        pltpu.make_async_copy(query_hbm, query, small_sem.at[1]),
        pltpu.make_async_copy(offset_hbm, offset, small_sem.at[2]),
    )

    barrier = pltpu.get_barrier_semaphore()
    below = (at.plane > 0).astype(jnp.int32)
    above = (at.plane < at.planes - 1).astype(jnp.int32)

    def signal_column(semaphore):
        @pl.when(below == 1)
        def _():
            pl.semaphore_signal(
                semaphore, inc=1, device_id=(at.seq - at.sides, at.group), device_id_type=MESH
            )

        @pl.when(above == 1)
        def _():
            pl.semaphore_signal(
                semaphore, inc=1, device_id=(at.seq + at.sides, at.group), device_id_type=MESH
            )

    near = at.near_half()
    x_copy(near).start()
    small_copies[0].start()
    w_copy(0, 0).start()
    w_copy(0, 1).start()
    signal_column(barrier)

    @pl.loop(0, at.per_plane)
    def _(peer):
        device = at.plane * at.per_plane + peer

        @pl.when(device != me)
        def _():
            pl.semaphore_signal(
                barrier,
                inc=1,
                device_id=(device // groups, lax.rem(device, groups)),
                device_id_type=MESH,
            )

    x_copy(near).wait()
    small_copies[0].wait()
    for turn in range(1, groups):
        w_copy(turn, 0).start()
        w_copy(turn, 1).start()
    small_copies[1].start()
    small_copies[2].start()

    @pl.loop(0, seqs)
    def _(half):
        @pl.when(half != near)
        def _():
            x_copy(half).start()

    rounds = at.planes - 1
    if rounds == 0:
        pl.semaphore_wait(barrier, at.per_plane - 1)
    else:
        pl.semaphore_wait(barrier, at.per_plane - 1 + below + above)
        signal_column(round_sem.at[0])

    def finish_round(number):
        pl.semaphore_wait(round_sem.at[number], below + above)
        if number + 1 < rounds:
            signal_column(round_sem.at[number + 1])

    def block_rows(device):
        return pl.ds(pl.multiple_of(device * positions, positions), positions)

    def remote(half, turn, part):
        seq = at.send_seq(half)
        group = at.send_group(turn)
        device = seq * groups + group
        cols = pl.ds(part * columns, columns)
        return device, pltpu.make_async_remote_copy(
            src_ref=outgoing.at[half, turn, :, cols],
            dst_ref=arrived.at[block_rows(me), cols],
            send_sem=send_sem.at[device],
            recv_sem=recv_sem.at[me],
            device_id=(seq, group),
            device_id_type=MESH,
        )

    def launch(half, turn, part):
        device, copy = remote(half, turn, part)

        @pl.when(device != me)
        def _():
            copy.start()

        @pl.when(device == me)
        def _():
            cols = slice(part * columns, (part + 1) * columns)
            arrived[block_rows(me), cols] = outgoing[half, turn, :, cols]

    def norm(half):
        @pl.loop(0, positions // NORM_ROWS)
        def _(chunk):
            rows = pl.ds(pl.multiple_of(chunk * NORM_ROWS, NORM_ROWS), NORM_ROWS)
            squares = jnp.zeros((NORM_ROWS, LANES), jnp.float32)
            for first in range(0, width, LANES):
                wide = x_buf[half, rows, first : first + LANES].astype(jnp.float32)
                squares = squares + wide * wide
            scale = lax.rsqrt(jnp.sum(squares, axis=-1, keepdims=True) / width + norm_epsilon)
            for first in range(0, width, LANES):
                cols = slice(first, first + LANES)
                wide = x_buf[half, rows, cols].astype(jnp.float32)
                normed[rows, cols] = (
                    wide * scale * gain[cols].astype(jnp.float32).reshape(1, LANES)
                ).astype(jnp.bfloat16)

    def project(half, turn, part):
        weight = (key_w, value_w)[part]
        outgoing[half, turn, :, part * columns : (part + 1) * columns] = jnp.dot(
            normed[...], weight[turn], preferred_element_type=jnp.float32
        ).astype(jnp.bfloat16)

    @pl.loop(0, devices)
    def _(index):
        half, turn = at.place(index)

        @pl.when((turn == 0) & (half != near))
        def _():
            x_copy(half).wait()

        @pl.when((turn == 0) | (index == EARLY) | ((half == near) & (turn == EARLY)))
        def _():
            norm(half)

        fresh = (index < EARLY) | ((index < EARLY + groups) & (turn >= EARLY))

        @pl.when(fresh)
        def _():
            w_copy(turn, 0).wait()

        project(half, turn, 0)

        @pl.when(index > 0)
        def _():
            last_half, last_turn = at.place(index - 1)
            launch(last_half, last_turn, 1)

        @pl.when(fresh)
        def _():
            w_copy(turn, 1).wait()

        project(half, turn, 1)
        for number in range(rounds):

            @pl.when(index == min(number, EARLY))
            def _():
                finish_round(number)

        launch(half, turn, 0)

    small_copies[1].wait()
    small_copies[2].wait()
    row = lax.broadcasted_iota(jnp.int32, (pad, columns), 0)
    col = lax.broadcasted_iota(jnp.int32, (pad, columns), 1)
    masked_query[...] = jnp.where(
        row == col // head_dim,
        jnp.broadcast_to(query[...].astype(jnp.float32), (pad, columns)),
        0.0,
    ).astype(jnp.bfloat16)
    score_row = lax.broadcasted_iota(jnp.int32, (pad, positions), 0)
    head_offsets = jnp.zeros((pad, positions), jnp.float32)
    for head in range(local_heads):
        head_offsets = jnp.where(
            score_row == head, offset[at.group * local_heads + head], head_offsets
        )
    offsets[...] = head_offsets
    last_half, last_turn = at.place(jnp.int32(devices - 1))
    launch(last_half, last_turn, 1)

    earlier = later_matrix(positions)

    def wait_block(source):
        @pl.when(source != me)
        def _():
            pltpu.make_async_copy(
                outgoing.at[0, 0], arrived.at[block_rows(source)], recv_sem.at[source]
            ).wait()

    @pl.loop(0, devices // BATCH - 1)
    def _(batch):
        sources = [at.source(batch * BATCH + k) for k in range(BATCH)]
        for source in sources:
            wait_block(source)
        for source in sources:
            rows = block_rows(source)
            reading, rest = read_block(
                masked_query[...],
                offsets[...],
                earlier,
                arrived[rows, :columns],
                arrived[rows, columns:],
                head_dim,
            )
            block_read[source] = reading
            block_rest[source] = rest

    @pl.loop(0, devices)
    def _(index):
        half = index // groups
        turn = lax.rem(index, groups)
        device = at.send_seq(half) * groups + at.send_group(turn)

        @pl.when(device != me)
        def _():
            pltpu.make_async_copy(
                outgoing.at[half, turn], arrived.at[block_rows(device)], send_sem.at[device]
            ).wait()

    for k in range(BATCH):
        wait_block(at.source(jnp.int32(devices - BATCH + k)))


def finish_kernel(
    seqs,
    groups,
    local_heads,
    arrived,
    block_read,
    block_rest,
    masked_query,
    offsets,
    keys_hbm,
    values_hbm,
    read_hbm,
    last_read,
    last_rest,
    read,
    out_sem,
    read_sem,
):
    devices = seqs * groups
    length = arrived.shape[0]
    positions = length // devices
    columns = masked_query.shape[1]
    head_dim = columns // local_heads
    at = Layout(seqs, groups)
    pieces = out_sem.shape[1]
    span = length // pieces

    def out_copies(piece):
        rows = pl.ds(piece * span, span)
        return (
            pltpu.make_async_copy(
                arrived.at[rows, pl.ds(0, columns)], keys_hbm.at[rows], out_sem.at[0, piece]
            ),
            pltpu.make_async_copy(
                arrived.at[rows, pl.ds(columns, columns)], values_hbm.at[rows], out_sem.at[1, piece]
            ),
        )

    for piece in range(pieces):
        for copy in out_copies(piece):
            copy.start()

    sources = [at.source(jnp.int32(devices - BATCH + k)) for k in range(BATCH)]
    earlier = later_matrix(positions)
    last_read[...] = block_read[...]
    last_rest[...] = block_rest[...]
    for source in sources:
        rows = pl.ds(pl.multiple_of(source * positions, positions), positions)
        reading, rest = read_block(
            masked_query[...],
            offsets[...],
            earlier,
            arrived[rows, :columns],
            arrived[rows, columns:],
            head_dim,
        )
        last_read[source] = reading
        last_rest[source] = rest

    reading = jnp.zeros(last_read.shape[1:], jnp.float32)
    after = jnp.zeros(last_rest.shape[1:], jnp.float32)
    for device in reversed(range(devices)):
        scale = jnp.exp(after)
        reading = reading + jnp.concatenate([scale] * (columns // positions), axis=1) * last_read[device]
        after = after + last_rest[device]
    for head in range(local_heads):
        own_cols = slice(head * head_dim, (head + 1) * head_dim)
        part = reading[head : head + 1, own_cols]
        read[:, own_cols] = part * lax.rsqrt(
            jnp.mean(part * part, axis=-1, keepdims=True) + norm_epsilon
        )
    read_copy = pltpu.make_async_copy(read, read_hbm, read_sem)
    read_copy.start(priority=1)
    for piece in range(pieces):
        for copy in out_copies(piece):
            copy.wait()
    read_copy.wait()


def shards(seqs, groups, layer_input, norm_gain, key_weight, value_weight, new_query, score_offset):
    seq_count, positions, width = layer_input.shape
    columns = new_query.shape[1]
    local_heads = score_offset.shape[0] // groups
    pad = -(-local_heads // 8) * 8
    devices = seqs * groups
    length = devices * positions
    hbm = pl.BlockSpec(memory_space=pltpu.HBM)
    vmem = pl.BlockSpec(memory_space=pltpu.VMEM)
    passed_bytes = 4 * length * columns + 4 * devices * pad * (columns + positions)
    passed = pl.pallas_call(
        functools.partial(exchange_kernel, seqs, groups, local_heads),
        out_shape=(
            pltpu.VMEM((length, 2 * columns), jnp.bfloat16),
            pltpu.VMEM((devices, pad, columns), jnp.float32),
            pltpu.VMEM((devices, pad, positions), jnp.float32),
            pltpu.VMEM((pad, columns), jnp.bfloat16),
            pltpu.VMEM((pad, positions), jnp.float32),
        ),
        in_specs=[hbm] * 6,
        out_specs=(vmem,) * 5,
        scratch_shapes=[
            pltpu.VMEM((seq_count, positions, width), jnp.bfloat16),
            pltpu.VMEM((width,), jnp.bfloat16),
            pltpu.VMEM((1, columns), jnp.bfloat16),
            pltpu.SMEM(score_offset.shape, jnp.float32),
            pltpu.VMEM((positions, width), jnp.bfloat16),
            pltpu.VMEM((groups, width, columns), jnp.bfloat16),
            pltpu.VMEM((groups, width, columns), jnp.bfloat16),
            pltpu.VMEM((seqs, groups, positions, 2 * columns), jnp.bfloat16),
            pltpu.SemaphoreType.DMA((seq_count,)),
            pltpu.SemaphoreType.DMA((2, groups)),
            pltpu.SemaphoreType.DMA((3,)),
            pltpu.SemaphoreType.DMA((devices,)),
            pltpu.SemaphoreType.DMA((devices,)),
            pltpu.SemaphoreType.REGULAR((seqs,)),
        ],
        compiler_params=pltpu.CompilerParams(
            collective_id=0, has_side_effects=True, vmem_limit_bytes=VMEM_BYTES - passed_bytes
        ),
    )(layer_input, norm_gain, key_weight, value_weight, new_query, score_offset)
    keys, values, read = pl.pallas_call(
        functools.partial(finish_kernel, seqs, groups, local_heads),
        out_shape=(
            jax.ShapeDtypeStruct((length, columns), jnp.bfloat16),
            jax.ShapeDtypeStruct((length, columns), jnp.bfloat16),
            jax.ShapeDtypeStruct((1, columns), jnp.float32),
        ),
        in_specs=[vmem] * 5,
        out_specs=(hbm,) * 3,
        scratch_shapes=[
            pltpu.VMEM((devices, pad, columns), jnp.float32),
            pltpu.VMEM((devices, pad, positions), jnp.float32),
            pltpu.VMEM((1, columns), jnp.float32),
            pltpu.SemaphoreType.DMA((2, 4)),
            pltpu.SemaphoreType.DMA,
        ],
        compiler_params=pltpu.CompilerParams(vmem_limit_bytes=20000000),
    )(*passed)
    return (keys[None], values[None], read)


def solution(mesh):
    seqs = mesh.shape["sp"]
    groups = mesh.shape["tp"]
    placed = (P(None, ("sp", "tp"), None), P(), P(), P(), P("sp", "tp"), P())
    return jax.shard_map(
        functools.partial(shards, seqs, groups),
        mesh=mesh,
        in_specs=placed,
        out_specs=(P("sp", None, "tp"), P("sp", None, "tp"), P("sp", "tp")),
        check_vma=False,
    )
```

```python
import functools

import jax
import jax.numpy as jnp
from jax import lax
from jax.experimental import pallas as pl
from jax.experimental.pallas import tpu as pltpu
from jax.sharding import PartitionSpec as P

norm_epsilon = 1e-06
MESH = pl.DeviceIdType.MESH
NORM_ROWS = 64
LANES = 128
BATCH = 4
EARLY = 2
LAG = 2
VMEM_BYTES = 64000000


class Layout:
    def __init__(self, seqs, groups):
        self.seqs = seqs
        self.groups = groups
        self.sides = 2 if seqs % 2 == 0 else 1
        self.cores = 2 if groups % 2 == 0 else 1
        self.planes = seqs // self.sides
        self.ranks = groups // self.cores
        self.per_plane = self.sides * groups
        seq = lax.axis_index("sp")
        group = lax.axis_index("tp")
        self.me = seq * groups + group
        self.seq = seq
        self.group = group
        self.side = lax.rem(seq, self.sides)
        self.plane = seq // self.sides
        self.core = lax.rem(group, self.cores)
        self.rank = group // self.cores
        self.upper = (2 * self.plane >= self.planes).astype(jnp.int32)
        self.inner = self.plane + 1 - 2 * self.upper
        self.outer = self.plane - 1 + 2 * self.upper
        self.has_outer = (self.outer >= 0) & (self.outer < self.planes)
        self.is_middle = (2 * self.inner >= self.planes) != (self.upper == 1)

    def far_plane(self, step):
        return self.upper * step + (1 - self.upper) * (self.planes - 1 - step)

    def send_seq(self, half):
        side = lax.rem(self.side + half + self.core, self.sides)
        return self.far_plane(half // self.sides) * self.sides + side

    def near_half(self):
        step = jnp.int32(0)
        if self.planes > 1:
            step = self.upper * (self.plane - 1) + (1 - self.upper) * (self.planes - 2 - self.plane)
        return step * self.sides + self.straight()

    def straight(self):
        return lax.rem(self.sides - self.core, self.sides)

    def place(self, index):
        first = self.near_half() * self.groups
        late = index - EARLY
        late = late + EARLY * (late >= first).astype(jnp.int32)
        number = jnp.where(index < EARLY, first + index, late)
        return number // self.groups, lax.rem(number, self.groups)

    def send_group(self, turn):
        rank = lax.rem(self.rank + turn // self.cores, self.ranks)
        return rank * self.cores + lax.rem(self.core + turn, self.cores)

    def source_plane(self, step):
        near = self.planes - self.planes // 2
        plane = self.upper * (self.planes - 1 - self.plane) + (1 - self.upper) * self.plane
        first = lax.rem(plane + step, near)
        later = self.planes - 1 - (step - near)
        is_near = (step < near).astype(jnp.int32)
        plane = is_near * first + (1 - is_near) * later
        return self.upper * (self.planes - 1 - plane) + (1 - self.upper) * plane

    def source(self, index):
        within = lax.rem(index, self.per_plane)
        turn = lax.rem(within, self.groups)
        core = lax.rem(self.core + self.cores - lax.rem(turn, self.cores), self.cores)
        flip = lax.rem(within // self.groups + core, self.sides)
        side = lax.rem(self.side + self.sides - flip, self.sides)
        rank = lax.rem(self.rank + self.ranks - turn // self.cores, self.ranks)
        plane = self.source_plane(index // self.per_plane)
        return (plane * self.sides + side) * self.groups + rank * self.cores + core


def read_block(query, offsets, earlier, keys, values, head_dim):
    scores = lax.dot_general(
        query, keys, (((1,), (1,)), ((), ())), preferred_element_type=jnp.float32
    )
    scores = scores * head_dim ** (-0.5) + offsets
    soft = jnp.log1p(jnp.exp(-jnp.abs(scores)))
    rest = -jnp.maximum(scores, 0.0) - soft
    positions = scores.shape[1]
    sums = jnp.zeros((scores.shape[0], 2 * positions), jnp.float32)
    left = rest
    for _ in range(3):
        piece = left.astype(jnp.bfloat16)
        left = left - piece.astype(jnp.float32)
        sums = sums + jnp.dot(piece, earlier, preferred_element_type=jnp.float32)
    later = sums[:, :positions]
    weights = jnp.exp(jnp.minimum(scores, 0.0) - soft + later).astype(jnp.bfloat16)
    reading = jnp.dot(weights, values, preferred_element_type=jnp.float32)
    return reading, sums[:, positions:]


def later_matrix(positions):
    row = lax.broadcasted_iota(jnp.int32, (positions, 2 * positions), 0)
    col = lax.broadcasted_iota(jnp.int32, (positions, 2 * positions), 1)
    return ((row > col) | (col >= positions)).astype(jnp.float32).astype(jnp.bfloat16)


def exchange_kernel(
    seqs,
    groups,
    local_heads,
    x_hbm,
    gain_hbm,
    key_w_hbm,
    value_w_hbm,
    query_hbm,
    offset_hbm,
    arrived,
    block_read,
    block_rest,
    masked_query,
    offsets,
    x_buf,
    gain,
    query,
    offset,
    normed,
    key_w,
    value_w,
    outgoing,
    x_sem,
    w_sem,
    small_sem,
    send_sem,
    recv_sem,
    round_sem,
):
    positions = x_buf.shape[1]
    width = x_buf.shape[2]
    columns = query.shape[1]
    head_dim = columns // local_heads
    pad = masked_query.shape[0]
    devices = seqs * groups
    at = Layout(seqs, groups)
    me = at.me

    def x_copy(half):
        return pltpu.make_async_copy(x_hbm.at[at.send_seq(half)], x_buf.at[half], x_sem.at[half])

    def w_copy(turn, part):
        group = at.send_group(turn)
        cols = pl.ds(pl.multiple_of(group * columns, columns), columns)
        source = (key_w_hbm, value_w_hbm)[part].at[:, cols]
        return pltpu.make_async_copy(source, (key_w, value_w)[part].at[turn], w_sem.at[part, turn])

    small_copies = (
        pltpu.make_async_copy(gain_hbm, gain, small_sem.at[0]),
        pltpu.make_async_copy(query_hbm, query, small_sem.at[1]),
        pltpu.make_async_copy(offset_hbm, offset, small_sem.at[2]),
    )

    barrier = pltpu.get_barrier_semaphore()

    def signal(semaphore, plane, side, rank, core):
        pl.semaphore_signal(
            semaphore,
            inc=1,
            device_id=(plane * at.sides + side, rank * at.cores + core),
            device_id_type=MESH,
        )

    def signal_sides(semaphore, cores):
        for step in range(1, at.sides):
            for core in cores:
                signal(semaphore, at.plane, lax.rem(at.side + step, at.sides), at.rank, core)

    def signal_inner(semaphore):
        signal(semaphore, at.inner, at.side, at.rank, at.core)

    def signal_outer(semaphore):
        @pl.when(at.has_outer)
        def _():
            signal(semaphore, at.outer, at.side, at.rank, at.core)

    def greet():
        if at.planes > 1:

            @pl.when(at.is_middle)
            def _():
                for core in range(at.cores):
                    signal(barrier, at.inner, at.side, at.rank, core)

            @pl.when(at.has_outer)
            def _():
                for core in range(at.cores):
                    signal(barrier, at.outer, at.side, at.rank, core)

        cores = range(at.cores)
        signal_sides(barrier, cores)
        for step in range(1, at.ranks):
            for core in cores:
                signal(barrier, at.plane, at.side, lax.rem(at.rank + step, at.ranks), core)
        for step in range(1, at.cores):
            signal(barrier, at.plane, at.side, at.rank, lax.rem(at.core + step, at.cores))

    def meet():
        columns_met = at.sides + at.ranks - 1 + (at.planes > 1)
        pl.semaphore_wait(barrier, columns_met * at.cores - 1)
        signal_sides(round_sem.at[0], (at.core,))

    def pass_inwards():
        @pl.when(at.is_middle)
        def _():
            signal_inner(round_sem.at[2])

        @pl.when(jnp.logical_not(at.is_middle))
        def _():
            signal_inner(round_sem.at[1])

    def meet_plane():
        pl.semaphore_wait(round_sem.at[0], at.sides - 1)
        if at.planes > 1:
            pl.when(jnp.logical_not(at.has_outer))(pass_inwards)

    def meet_outer():
        if at.planes > 1:

            @pl.when(at.has_outer)
            def _():
                pl.semaphore_wait(round_sem.at[1], 1)
                pass_inwards()

    def meet_planes():
        if at.planes > 1:

            @pl.when(at.is_middle)
            def _():
                pl.semaphore_wait(round_sem.at[2], 1)

            @pl.when(jnp.logical_not(at.is_middle))
            def _():
                pl.semaphore_wait(round_sem.at[3], 1)

            signal_outer(round_sem.at[3])

    near = at.near_half()
    x_copy(near).start()
    small_copies[0].start()
    w_copy(0, 0).start()
    w_copy(0, 1).start()
    greet()
    x_copy(near).wait()
    small_copies[0].wait()
    for turn in range(1, groups):
        w_copy(turn, 0).start()
        w_copy(turn, 1).start()
    small_copies[1].start()
    small_copies[2].start()

    @pl.loop(0, seqs)
    def _(half):
        @pl.when(half != near)
        def _():
            x_copy(half).start()

    def block_rows(device):
        return pl.ds(pl.multiple_of(device * positions, positions), positions)

    def remote(half, turn, part):
        seq = at.send_seq(half)
        group = at.send_group(turn)
        device = seq * groups + group
        cols = pl.ds(part * columns, columns)
        return device, pltpu.make_async_remote_copy(
            src_ref=outgoing.at[half, turn, :, cols],
            dst_ref=arrived.at[block_rows(me), cols],
            send_sem=send_sem,
            recv_sem=recv_sem.at[at.plane * at.sides + lax.rem(half, at.sides)],
            device_id=(seq, group),
            device_id_type=MESH,
        )

    def launch(half, turn, part):
        device, copy = remote(half, turn, part)

        @pl.when(device != me)
        def _():
            copy.start()

        @pl.when(device == me)
        def _():
            cols = slice(part * columns, (part + 1) * columns)
            arrived[block_rows(me), cols] = outgoing[half, turn, :, cols]

    def launch_both(index):
        half, turn = at.place(index)
        launch(half, turn, 0)
        launch(half, turn, 1)

    def norm(half):
        @pl.loop(0, positions // NORM_ROWS)
        def _(chunk):
            rows = pl.ds(pl.multiple_of(chunk * NORM_ROWS, NORM_ROWS), NORM_ROWS)
            squares = jnp.zeros((NORM_ROWS, LANES), jnp.float32)
            for first in range(0, width, LANES):
                wide = x_buf[half, rows, first : first + LANES].astype(jnp.float32)
                squares = squares + wide * wide
            scale = lax.rsqrt(jnp.sum(squares, axis=-1, keepdims=True) / width + norm_epsilon)
            for first in range(0, width, LANES):
                cols = slice(first, first + LANES)
                wide = x_buf[half, rows, cols].astype(jnp.float32)
                normed[rows, cols] = (
                    wide * scale * gain[cols].astype(jnp.float32).reshape(1, LANES)
                ).astype(jnp.bfloat16)

    def project(half, turn, part):
        weight = (key_w, value_w)[part]
        outgoing[half, turn, :, part * columns : (part + 1) * columns] = jnp.dot(
            normed[...], weight[turn], preferred_element_type=jnp.float32
        ).astype(jnp.bfloat16)

    stages = (meet_plane, meet_outer, meet_planes)

    @pl.loop(0, devices)
    def _(index):
        half, turn = at.place(index)

        @pl.when((turn == 0) & (half != near))
        def _():
            x_copy(half).wait()

        @pl.when((turn == 0) | (index == EARLY) | ((half == near) & (turn == EARLY)))
        def _():
            norm(half)

        fresh = (index < EARLY) | ((index < EARLY + groups) & (turn >= EARLY))

        @pl.when(fresh)
        def _():
            w_copy(turn, 0).wait()

        project(half, turn, 0)

        @pl.when(index == 0)
        def _():
            meet()

        @pl.when((index > 0) & (index <= EARLY))
        def _():
            early_half, early_turn = at.place(index - 1)
            launch(early_half, early_turn, 1)

        @pl.when(fresh)
        def _():
            w_copy(turn, 1).wait()

        project(half, turn, 1)

        for number, stage in enumerate(stages):

            @pl.when(index == 2 + number)
            def _():
                stage()

        @pl.when(index < EARLY)
        def _():
            launch(half, turn, 0)

        @pl.when(index == EARLY + LAG)
        def _():
            @pl.loop(EARLY, EARLY + LAG)
            def _(number):
                launch_both(number)

        @pl.when(index > EARLY + LAG)
        def _():
            launch_both(index - 1)

    small_copies[1].wait()
    small_copies[2].wait()
    row = lax.broadcasted_iota(jnp.int32, (pad, columns), 0)
    col = lax.broadcasted_iota(jnp.int32, (pad, columns), 1)
    masked_query[...] = jnp.where(
        row == col // head_dim,
        jnp.broadcast_to(query[...].astype(jnp.float32), (pad, columns)),
        0.0,
    ).astype(jnp.bfloat16)
    score_row = lax.broadcasted_iota(jnp.int32, (pad, positions), 0)
    head_offsets = jnp.zeros((pad, positions), jnp.float32)
    for head in range(local_heads):
        head_offsets = jnp.where(
            score_row == head, offset[at.group * local_heads + head], head_offsets
        )
    offsets[...] = head_offsets
    launch_both(jnp.int32(devices - 1))

    earlier = later_matrix(positions)

    def wait_group(number):
        plane = at.source_plane(number // at.sides)
        half = lax.rem(number, at.sides)
        semaphore = recv_sem.at[plane * at.sides + half]

        def wait_blocks(count):
            whole = arrived.at[pl.ds(0, count * positions)]
            pltpu.make_async_copy(whole, whole, semaphore).wait()

        with_own = (plane == at.plane) & (half == at.straight())

        @pl.when(with_own)
        def _():
            wait_blocks(groups - 1)

        @pl.when(jnp.logical_not(with_own))
        def _():
            wait_blocks(groups)

    @pl.loop(0, seqs - 1)
    def _(number):
        wait_group(number)

        @pl.loop(0, groups // BATCH)
        def _(batch):
            for k in range(BATCH):
                source = at.source(number * groups + batch * BATCH + k)
                rows = block_rows(source)
                reading, rest = read_block(
                    masked_query[...],
                    offsets[...],
                    earlier,
                    arrived[rows, :columns],
                    arrived[rows, columns:],
                    head_dim,
                )
                block_read[source] = reading
                block_rest[source] = rest

    sent = arrived.at[pl.ds(0, (devices - 1) * positions)]
    pltpu.make_async_copy(sent, sent, send_sem).wait()
    wait_group(jnp.int32(seqs - 1))


def finish_kernel(
    seqs,
    groups,
    local_heads,
    arrived,
    block_read,
    block_rest,
    masked_query,
    offsets,
    keys_hbm,
    values_hbm,
    read_hbm,
    last_read,
    last_rest,
    read,
    out_sem,
    read_sem,
):
    devices = seqs * groups
    length = arrived.shape[0]
    positions = length // devices
    columns = masked_query.shape[1]
    head_dim = columns // local_heads
    at = Layout(seqs, groups)
    pieces = out_sem.shape[1]
    span = length // pieces

    def out_copies(piece):
        rows = pl.ds(pl.multiple_of(piece * span, span), span)
        return (
            pltpu.make_async_copy(
                arrived.at[rows, pl.ds(0, columns)], keys_hbm.at[rows], out_sem.at[0, piece]
            ),
            pltpu.make_async_copy(
                arrived.at[rows, pl.ds(columns, columns)], values_hbm.at[rows], out_sem.at[1, piece]
            ),
        )

    @pl.loop(0, pieces)
    def _(piece):
        for copy in out_copies(piece):
            copy.start()

    sources = [at.source(jnp.int32(devices - groups + k)) for k in range(groups)]
    earlier = later_matrix(positions)
    last_read[...] = block_read[...]
    last_rest[...] = block_rest[...]
    for source in sources:
        rows = pl.ds(pl.multiple_of(source * positions, positions), positions)
        reading, rest = read_block(
            masked_query[...],
            offsets[...],
            earlier,
            arrived[rows, :columns],
            arrived[rows, columns:],
            head_dim,
        )
        last_read[source] = reading
        last_rest[source] = rest

    reading = jnp.zeros(last_read.shape[1:], jnp.float32)
    after = jnp.zeros(last_rest.shape[1:], jnp.float32)
    for device in reversed(range(devices)):
        scale = jnp.exp(after)
        reading = reading + jnp.concatenate([scale] * (columns // positions), axis=1) * last_read[device]
        after = after + last_rest[device]
    for head in range(local_heads):
        own_cols = slice(head * head_dim, (head + 1) * head_dim)
        part = reading[head : head + 1, own_cols]
        read[:, own_cols] = part * lax.rsqrt(
            jnp.mean(part * part, axis=-1, keepdims=True) + norm_epsilon
        )
    read_copy = pltpu.make_async_copy(read, read_hbm, read_sem)
    read_copy.start(priority=1)
    @pl.loop(0, pieces)
    def _(piece):
        for copy in out_copies(piece):
            copy.wait()

    read_copy.wait()


def shards(seqs, groups, layer_input, norm_gain, key_weight, value_weight, new_query, score_offset):
    seq_count, positions, width = layer_input.shape
    columns = new_query.shape[1]
    local_heads = score_offset.shape[0] // groups
    pad = -(-local_heads // 8) * 8
    devices = seqs * groups
    length = devices * positions
    hbm = pl.BlockSpec(memory_space=pltpu.HBM)
    vmem = pl.BlockSpec(memory_space=pltpu.VMEM)
    passed_bytes = 4 * length * columns + 4 * devices * pad * (columns + positions)
    passed = pl.pallas_call(
        functools.partial(exchange_kernel, seqs, groups, local_heads),
        out_shape=(
            pltpu.VMEM((length, 2 * columns), jnp.bfloat16),
            pltpu.VMEM((devices, pad, columns), jnp.float32),
            pltpu.VMEM((devices, pad, positions), jnp.float32),
            pltpu.VMEM((pad, columns), jnp.bfloat16),
            pltpu.VMEM((pad, positions), jnp.float32),
        ),
        in_specs=[hbm] * 6,
        out_specs=(vmem,) * 5,
        scratch_shapes=[
            pltpu.VMEM((seq_count, positions, width), jnp.bfloat16),
            pltpu.VMEM((width,), jnp.bfloat16),
            pltpu.VMEM((1, columns), jnp.bfloat16),
            pltpu.SMEM(score_offset.shape, jnp.float32),
            pltpu.VMEM((positions, width), jnp.bfloat16),
            pltpu.VMEM((groups, width, columns), jnp.bfloat16),
            pltpu.VMEM((groups, width, columns), jnp.bfloat16),
            pltpu.VMEM((seqs, groups, positions, 2 * columns), jnp.bfloat16),
            pltpu.SemaphoreType.DMA((seq_count,)),
            pltpu.SemaphoreType.DMA((2, groups)),
            pltpu.SemaphoreType.DMA((3,)),
            pltpu.SemaphoreType.DMA,
            pltpu.SemaphoreType.DMA((seqs,)),
            pltpu.SemaphoreType.REGULAR((4,)),
        ],
        compiler_params=pltpu.CompilerParams(
            collective_id=0, has_side_effects=True, vmem_limit_bytes=VMEM_BYTES - passed_bytes
        ),
    )(layer_input, norm_gain, key_weight, value_weight, new_query, score_offset)
    keys, values, read = pl.pallas_call(
        functools.partial(finish_kernel, seqs, groups, local_heads),
        out_shape=(
            jax.ShapeDtypeStruct((length, columns), jnp.bfloat16),
            jax.ShapeDtypeStruct((length, columns), jnp.bfloat16),
            jax.ShapeDtypeStruct((1, columns), jnp.float32),
        ),
        in_specs=[vmem] * 5,
        out_specs=(hbm,) * 3,
        scratch_shapes=[
            pltpu.VMEM((devices, pad, columns), jnp.float32),
            pltpu.VMEM((devices, pad, positions), jnp.float32),
            pltpu.VMEM((1, columns), jnp.float32),
            pltpu.SemaphoreType.DMA((2, 4)),
            pltpu.SemaphoreType.DMA,
        ],
        compiler_params=pltpu.CompilerParams(vmem_limit_bytes=20000000),
    )(*passed)
    return (keys[None], values[None], read)


def solution(mesh):
    seqs = mesh.shape["sp"]
    groups = mesh.shape["tp"]
    placed = (P(None, ("sp", "tp"), None), P(), P(), P(), P("sp", "tp"), P())
    return jax.shard_map(
        functools.partial(shards, seqs, groups),
        mesh=mesh,
        in_specs=placed,
        out_specs=(P("sp", None, "tp"), P("sp", None, "tp"), P("sp", "tp")),
        check_vma=False,
    )
```

```python
import functools

import jax
import jax.numpy as jnp
from jax import lax
from jax.experimental import pallas as pl
from jax.experimental.pallas import tpu as pltpu
from jax.sharding import PartitionSpec as P

norm_epsilon = 1e-06
MESH = pl.DeviceIdType.MESH
NORM_ROWS = 64
LANES = 128
BATCH = 4
EARLY = 2
LAG = 2
VMEM_BYTES = 64000000


class Layout:
    def __init__(self, seqs, groups):
        self.seqs = seqs
        self.groups = groups
        self.sides = 2 if seqs % 2 == 0 else 1
        self.cores = 2 if groups % 2 == 0 else 1
        self.planes = seqs // self.sides
        self.ranks = groups // self.cores
        self.per_plane = self.sides * groups
        seq = lax.axis_index("sp")
        group = lax.axis_index("tp")
        self.me = seq * groups + group
        self.seq = seq
        self.group = group
        self.side = lax.rem(seq, self.sides)
        self.plane = seq // self.sides
        self.core = lax.rem(group, self.cores)
        self.rank = group // self.cores
        self.upper = (2 * self.plane >= self.planes).astype(jnp.int32)
        self.inner = self.plane + 1 - 2 * self.upper
        self.outer = self.plane - 1 + 2 * self.upper
        self.has_outer = (self.outer >= 0) & (self.outer < self.planes)
        self.is_middle = (2 * self.inner >= self.planes) != (self.upper == 1)

    def far_plane(self, step):
        return self.upper * step + (1 - self.upper) * (self.planes - 1 - step)

    def send_seq(self, half):
        side = lax.rem(self.side + half + self.core, self.sides)
        return self.far_plane(half // self.sides) * self.sides + side

    def near_half(self):
        step = jnp.int32(0)
        if self.planes > 1:
            step = self.upper * (self.plane - 1) + (1 - self.upper) * (self.planes - 2 - self.plane)
        return step * self.sides + self.straight()

    def straight(self):
        return lax.rem(self.sides - self.core, self.sides)

    def opens(self, index):
        first = self.near_half() * self.groups
        late = index - EARLY
        late = late + EARLY * (late >= first).astype(jnp.int32)
        return (index >= EARLY) & (lax.rem(late, self.groups) == 0)

    def place(self, index):
        first = self.near_half() * self.groups
        late = index - EARLY
        late = late + EARLY * (late >= first).astype(jnp.int32)
        number = jnp.where(index < EARLY, first + index, late)
        half = number // self.groups
        turn = lax.rem(number, self.groups)
        if self.planes > 2:
            last_half = self.near_half() - self.straight() + self.sides - 1
            turned = lax.rem(turn + self.cores * (self.ranks - self.rank), self.groups)
            turn = jnp.where((half == last_half) & (self.core == 0), turned, turn)
        return half, turn

    def send_group(self, turn):
        rank = lax.rem(self.rank + turn // self.cores, self.ranks)
        return rank * self.cores + lax.rem(self.core + turn, self.cores)

    def source_plane(self, step):
        near = self.planes - self.planes // 2
        plane = self.upper * (self.planes - 1 - self.plane) + (1 - self.upper) * self.plane
        first = lax.rem(plane + step, near)
        later = self.planes - 1 - (step - near)
        is_near = (step < near).astype(jnp.int32)
        plane = is_near * first + (1 - is_near) * later
        return self.upper * (self.planes - 1 - plane) + (1 - self.upper) * plane

    def source(self, index):
        within = lax.rem(index, self.per_plane)
        turn = lax.rem(within, self.groups)
        core = lax.rem(self.core + self.cores - lax.rem(turn, self.cores), self.cores)
        flip = lax.rem(within // self.groups + core, self.sides)
        side = lax.rem(self.side + self.sides - flip, self.sides)
        rank = lax.rem(self.rank + self.ranks - turn // self.cores, self.ranks)
        plane = self.source_plane(index // self.per_plane)
        return (plane * self.sides + side) * self.groups + rank * self.cores + core


def read_block(query, offsets, earlier, keys, values, head_dim):
    scores = lax.dot_general(
        query, keys, (((1,), (1,)), ((), ())), preferred_element_type=jnp.float32
    )
    scores = scores * head_dim ** (-0.5) + offsets
    soft = jnp.log1p(jnp.exp(-jnp.abs(scores)))
    rest = -jnp.maximum(scores, 0.0) - soft
    positions = scores.shape[1]
    sums = jnp.zeros((scores.shape[0], 2 * positions), jnp.float32)
    left = rest
    for _ in range(3):
        piece = left.astype(jnp.bfloat16)
        left = left - piece.astype(jnp.float32)
        sums = sums + jnp.dot(piece, earlier, preferred_element_type=jnp.float32)
    later = sums[:, :positions]
    weights = jnp.exp(jnp.minimum(scores, 0.0) - soft + later).astype(jnp.bfloat16)
    reading = jnp.dot(weights, values, preferred_element_type=jnp.float32)
    return reading, sums[:, positions:]


def later_matrix(positions):
    row = lax.broadcasted_iota(jnp.int32, (positions, 2 * positions), 0)
    col = lax.broadcasted_iota(jnp.int32, (positions, 2 * positions), 1)
    return ((row > col) | (col >= positions)).astype(jnp.float32).astype(jnp.bfloat16)


def exchange_kernel(
    seqs,
    groups,
    local_heads,
    x_hbm,
    gain_hbm,
    key_w_hbm,
    value_w_hbm,
    query_hbm,
    offset_hbm,
    arrived,
    block_read,
    block_rest,
    masked_query,
    offsets,
    x_buf,
    gain,
    query,
    offset,
    normed,
    key_w,
    value_w,
    outgoing,
    x_sem,
    w_sem,
    small_sem,
    send_sem,
    recv_sem,
    round_sem,
):
    positions = x_buf.shape[1]
    width = x_buf.shape[2]
    columns = query.shape[1]
    head_dim = columns // local_heads
    pad = masked_query.shape[0]
    devices = seqs * groups
    at = Layout(seqs, groups)
    me = at.me

    def x_copy(half):
        return pltpu.make_async_copy(x_hbm.at[at.send_seq(half)], x_buf.at[half], x_sem.at[half])

    def w_copy(turn, part):
        group = at.send_group(turn)
        cols = pl.ds(pl.multiple_of(group * columns, columns), columns)
        source = (key_w_hbm, value_w_hbm)[part].at[:, cols]
        return pltpu.make_async_copy(source, (key_w, value_w)[part].at[turn], w_sem.at[part, turn])

    small_copies = (
        pltpu.make_async_copy(gain_hbm, gain, small_sem.at[0]),
        pltpu.make_async_copy(query_hbm, query, small_sem.at[1]),
        pltpu.make_async_copy(offset_hbm, offset, small_sem.at[2]),
    )

    barrier = pltpu.get_barrier_semaphore()

    def signal(semaphore, plane, side, rank, core):
        pl.semaphore_signal(
            semaphore,
            inc=1,
            device_id=(plane * at.sides + side, rank * at.cores + core),
            device_id_type=MESH,
        )

    def signal_sides(semaphore, cores):
        for step in range(1, at.sides):
            for core in cores:
                signal(semaphore, at.plane, lax.rem(at.side + step, at.sides), at.rank, core)

    def signal_inner(semaphore):
        signal(semaphore, at.inner, at.side, at.rank, at.core)

    def signal_outer(semaphore):
        @pl.when(at.has_outer)
        def _():
            signal(semaphore, at.outer, at.side, at.rank, at.core)

    def greet():
        if at.planes > 1:

            @pl.when(at.is_middle)
            def _():
                for core in range(at.cores):
                    signal(barrier, at.inner, at.side, at.rank, core)

            @pl.when(at.has_outer)
            def _():
                for core in range(at.cores):
                    signal(barrier, at.outer, at.side, at.rank, core)

        cores = range(at.cores)
        signal_sides(barrier, cores)
        for step in range(1, at.ranks):
            for core in cores:
                signal(barrier, at.plane, at.side, lax.rem(at.rank + step, at.ranks), core)
        for step in range(1, at.cores):
            signal(barrier, at.plane, at.side, at.rank, lax.rem(at.core + step, at.cores))

    def meet():
        columns_met = at.sides + at.ranks - 1 + (at.planes > 1)
        pl.semaphore_wait(barrier, columns_met * at.cores - 1)
        signal_sides(round_sem.at[0], (at.core,))

    def pass_inwards():
        @pl.when(at.is_middle)
        def _():
            signal_inner(round_sem.at[2])

        @pl.when(jnp.logical_not(at.is_middle))
        def _():
            signal_inner(round_sem.at[1])

    def meet_plane():
        pl.semaphore_wait(round_sem.at[0], at.sides - 1)
        if at.planes > 1:
            pl.when(jnp.logical_not(at.has_outer))(pass_inwards)

    def meet_outer():
        if at.planes > 1:

            @pl.when(at.has_outer)
            def _():
                pl.semaphore_wait(round_sem.at[1], 1)
                pass_inwards()

    def meet_planes():
        if at.planes > 1:

            @pl.when(at.is_middle)
            def _():
                pl.semaphore_wait(round_sem.at[2], 1)

            @pl.when(jnp.logical_not(at.is_middle))
            def _():
                pl.semaphore_wait(round_sem.at[3], 1)

            signal_outer(round_sem.at[3])

    near = at.near_half()
    x_copy(near).start()
    small_copies[0].start()
    greet()
    w_copy(0, 0).start()
    w_copy(0, 1).start()
    x_copy(near).wait()
    small_copies[0].wait()
    for turn in range(1, groups):
        w_copy(turn, 0).start()
        w_copy(turn, 1).start()
    small_copies[1].start()
    small_copies[2].start()

    @pl.loop(0, seqs)
    def _(half):
        @pl.when(half != near)
        def _():
            x_copy(half).start()

    def block_rows(device):
        return pl.ds(pl.multiple_of(device * positions, positions), positions)

    def remote(half, turn, part):
        seq = at.send_seq(half)
        group = at.send_group(turn)
        device = seq * groups + group
        cols = pl.ds(part * columns, columns)
        return device, pltpu.make_async_remote_copy(
            src_ref=outgoing.at[half, turn, :, cols],
            dst_ref=arrived.at[block_rows(me), cols],
            send_sem=send_sem,
            recv_sem=recv_sem.at[at.plane * at.sides + lax.rem(half, at.sides)],
            device_id=(seq, group),
            device_id_type=MESH,
        )

    def launch(half, turn, part):
        device, copy = remote(half, turn, part)

        @pl.when(device != me)
        def _():
            copy.start()

        @pl.when(device == me)
        def _():
            cols = slice(part * columns, (part + 1) * columns)
            arrived[block_rows(me), cols] = outgoing[half, turn, :, cols]

    def launch_both(index):
        half, turn = at.place(index)
        launch(half, turn, 0)
        launch(half, turn, 1)

    def norm(half):
        @pl.loop(0, positions // NORM_ROWS)
        def _(chunk):
            rows = pl.ds(pl.multiple_of(chunk * NORM_ROWS, NORM_ROWS), NORM_ROWS)
            squares = jnp.zeros((NORM_ROWS, LANES), jnp.float32)
            for first in range(0, width, LANES):
                wide = x_buf[half, rows, first : first + LANES].astype(jnp.float32)
                squares = squares + wide * wide
            scale = lax.rsqrt(jnp.sum(squares, axis=-1, keepdims=True) / width + norm_epsilon)
            for first in range(0, width, LANES):
                cols = slice(first, first + LANES)
                wide = x_buf[half, rows, cols].astype(jnp.float32)
                normed[rows, cols] = (
                    wide * scale * gain[cols].astype(jnp.float32).reshape(1, LANES)
                ).astype(jnp.bfloat16)

    def project(half, turn, part):
        weight = (key_w, value_w)[part]
        outgoing[half, turn, :, part * columns : (part + 1) * columns] = jnp.dot(
            normed[...], weight[turn], preferred_element_type=jnp.float32
        ).astype(jnp.bfloat16)

    stages = (meet_plane, meet_outer, meet_planes)

    @pl.loop(0, devices)
    def _(index):
        half, turn = at.place(index)
        opens = at.opens(index)

        @pl.when(opens & (half != near))
        def _():
            x_copy(half).wait()

        @pl.when(opens | (index == 0) | (index == EARLY) | ((half == near) & (turn == EARLY)))
        def _():
            norm(half)

        fresh = (index < EARLY) | ((index < EARLY + groups) & (turn >= EARLY))

        @pl.when(fresh)
        def _():
            w_copy(turn, 0).wait()

        project(half, turn, 0)

        @pl.when(index == 0)
        def _():
            meet()
            launch(half, turn, 0)

        @pl.when((index > 0) & (index <= EARLY))
        def _():
            early_half, early_turn = at.place(index - 1)
            launch(early_half, early_turn, 1)

        @pl.when(fresh)
        def _():
            w_copy(turn, 1).wait()

        project(half, turn, 1)

        for number, stage in enumerate(stages):

            @pl.when(index == 2 + number)
            def _():
                stage()

        @pl.when((index > 0) & (index < EARLY))
        def _():
            launch(half, turn, 0)

        @pl.when(index == EARLY + LAG)
        def _():
            @pl.loop(EARLY, EARLY + LAG)
            def _(number):
                launch_both(number)

        @pl.when(index > EARLY + LAG)
        def _():
            launch_both(index - 1)

    small_copies[1].wait()
    small_copies[2].wait()
    row = lax.broadcasted_iota(jnp.int32, (pad, columns), 0)
    col = lax.broadcasted_iota(jnp.int32, (pad, columns), 1)
    masked_query[...] = jnp.where(
        row == col // head_dim,
        jnp.broadcast_to(query[...].astype(jnp.float32), (pad, columns)),
        0.0,
    ).astype(jnp.bfloat16)
    score_row = lax.broadcasted_iota(jnp.int32, (pad, positions), 0)
    head_offsets = jnp.zeros((pad, positions), jnp.float32)
    for head in range(local_heads):
        head_offsets = jnp.where(
            score_row == head, offset[at.group * local_heads + head], head_offsets
        )
    offsets[...] = head_offsets
    launch_both(jnp.int32(devices - 1))

    earlier = later_matrix(positions)

    def wait_group(number):
        plane = at.source_plane(number // at.sides)
        half = lax.rem(number, at.sides)
        semaphore = recv_sem.at[plane * at.sides + half]

        def wait_blocks(count):
            whole = arrived.at[pl.ds(0, count * positions)]
            pltpu.make_async_copy(whole, whole, semaphore).wait()

        with_own = (plane == at.plane) & (half == at.straight())

        @pl.when(with_own)
        def _():
            wait_blocks(groups - 1)

        @pl.when(jnp.logical_not(with_own))
        def _():
            wait_blocks(groups)

    @pl.loop(0, seqs - 1)
    def _(number):
        wait_group(number)

        @pl.loop(0, groups // BATCH)
        def _(batch):
            for k in range(BATCH):
                source = at.source(number * groups + batch * BATCH + k)
                rows = block_rows(source)
                reading, rest = read_block(
                    masked_query[...],
                    offsets[...],
                    earlier,
                    arrived[rows, :columns],
                    arrived[rows, columns:],
                    head_dim,
                )
                block_read[source] = reading
                block_rest[source] = rest

    sent = arrived.at[pl.ds(0, (devices - 1) * positions)]
    pltpu.make_async_copy(sent, sent, send_sem).wait()
    wait_group(jnp.int32(seqs - 1))


def finish_kernel(
    seqs,
    groups,
    local_heads,
    arrived,
    block_read,
    block_rest,
    masked_query,
    offsets,
    keys_hbm,
    values_hbm,
    read_hbm,
    last_read,
    last_rest,
    read,
    out_sem,
    read_sem,
):
    devices = seqs * groups
    length = arrived.shape[0]
    positions = length // devices
    columns = masked_query.shape[1]
    head_dim = columns // local_heads
    at = Layout(seqs, groups)
    pieces = out_sem.shape[1]
    span = length // pieces

    def out_copies(piece):
        rows = pl.ds(pl.multiple_of(piece * span, span), span)
        return (
            pltpu.make_async_copy(
                arrived.at[rows, pl.ds(0, columns)], keys_hbm.at[rows], out_sem.at[0, piece]
            ),
            pltpu.make_async_copy(
                arrived.at[rows, pl.ds(columns, columns)], values_hbm.at[rows], out_sem.at[1, piece]
            ),
        )

    @pl.loop(0, pieces)
    def _(piece):
        for copy in out_copies(piece):
            copy.start()

    sources = [at.source(jnp.int32(devices - groups + k)) for k in range(groups)]
    earlier = later_matrix(positions)
    last_read[...] = block_read[...]
    last_rest[...] = block_rest[...]
    for source in sources:
        rows = pl.ds(pl.multiple_of(source * positions, positions), positions)
        reading, rest = read_block(
            masked_query[...],
            offsets[...],
            earlier,
            arrived[rows, :columns],
            arrived[rows, columns:],
            head_dim,
        )
        last_read[source] = reading
        last_rest[source] = rest

    reading = jnp.zeros(last_read.shape[1:], jnp.float32)
    after = jnp.zeros(last_rest.shape[1:], jnp.float32)
    for device in reversed(range(devices)):
        scale = jnp.exp(after)
        reading = reading + jnp.concatenate([scale] * (columns // positions), axis=1) * last_read[device]
        after = after + last_rest[device]
    for head in range(local_heads):
        own_cols = slice(head * head_dim, (head + 1) * head_dim)
        part = reading[head : head + 1, own_cols]
        read[:, own_cols] = part * lax.rsqrt(
            jnp.mean(part * part, axis=-1, keepdims=True) + norm_epsilon
        )
    read_copy = pltpu.make_async_copy(read, read_hbm, read_sem)
    read_copy.start(priority=1)
    @pl.loop(0, pieces)
    def _(piece):
        for copy in out_copies(piece):
            copy.wait()

    read_copy.wait()


def shards(seqs, groups, layer_input, norm_gain, key_weight, value_weight, new_query, score_offset):
    seq_count, positions, width = layer_input.shape
    columns = new_query.shape[1]
    local_heads = score_offset.shape[0] // groups
    pad = -(-local_heads // 8) * 8
    devices = seqs * groups
    length = devices * positions
    hbm = pl.BlockSpec(memory_space=pltpu.HBM)
    vmem = pl.BlockSpec(memory_space=pltpu.VMEM)
    passed_bytes = 4 * length * columns + 4 * devices * pad * (columns + positions)
    passed = pl.pallas_call(
        functools.partial(exchange_kernel, seqs, groups, local_heads),
        out_shape=(
            pltpu.VMEM((length, 2 * columns), jnp.bfloat16),
            pltpu.VMEM((devices, pad, columns), jnp.float32),
            pltpu.VMEM((devices, pad, positions), jnp.float32),
            pltpu.VMEM((pad, columns), jnp.bfloat16),
            pltpu.VMEM((pad, positions), jnp.float32),
        ),
        in_specs=[hbm] * 6,
        out_specs=(vmem,) * 5,
        scratch_shapes=[
            pltpu.VMEM((seq_count, positions, width), jnp.bfloat16),
            pltpu.VMEM((width,), jnp.bfloat16),
            pltpu.VMEM((1, columns), jnp.bfloat16),
            pltpu.SMEM(score_offset.shape, jnp.float32),
            pltpu.VMEM((positions, width), jnp.bfloat16),
            pltpu.VMEM((groups, width, columns), jnp.bfloat16),
            pltpu.VMEM((groups, width, columns), jnp.bfloat16),
            pltpu.VMEM((seqs, groups, positions, 2 * columns), jnp.bfloat16),
            pltpu.SemaphoreType.DMA((seq_count,)),
            pltpu.SemaphoreType.DMA((2, groups)),
            pltpu.SemaphoreType.DMA((3,)),
            pltpu.SemaphoreType.DMA,
            pltpu.SemaphoreType.DMA((seqs,)),
            pltpu.SemaphoreType.REGULAR((4,)),
        ],
        compiler_params=pltpu.CompilerParams(
            collective_id=0, has_side_effects=True, vmem_limit_bytes=VMEM_BYTES - passed_bytes
        ),
    )(layer_input, norm_gain, key_weight, value_weight, new_query, score_offset)
    keys, values, read = pl.pallas_call(
        functools.partial(finish_kernel, seqs, groups, local_heads),
        out_shape=(
            jax.ShapeDtypeStruct((length, columns), jnp.bfloat16),
            jax.ShapeDtypeStruct((length, columns), jnp.bfloat16),
            jax.ShapeDtypeStruct((1, columns), jnp.float32),
        ),
        in_specs=[vmem] * 5,
        out_specs=(hbm,) * 3,
        scratch_shapes=[
            pltpu.VMEM((devices, pad, columns), jnp.float32),
            pltpu.VMEM((devices, pad, positions), jnp.float32),
            pltpu.VMEM((1, columns), jnp.float32),
            pltpu.SemaphoreType.DMA((2, 4)),
            pltpu.SemaphoreType.DMA,
        ],
        compiler_params=pltpu.CompilerParams(vmem_limit_bytes=20000000),
    )(*passed)
    return (keys[None], values[None], read)


def solution(mesh):
    seqs = mesh.shape["sp"]
    groups = mesh.shape["tp"]
    placed = (P(None, ("sp", "tp"), None), P(), P(), P(), P("sp", "tp"), P())
    return jax.shard_map(
        functools.partial(shards, seqs, groups),
        mesh=mesh,
        in_specs=placed,
        out_specs=(P("sp", None, "tp"), P("sp", None, "tp"), P("sp", "tp")),
        check_vma=False,
    )
```

```python
import functools

import jax
import jax.numpy as jnp
from jax import lax
from jax.experimental import pallas as pl
from jax.experimental.pallas import tpu as pltpu
from jax.sharding import PartitionSpec as P

norm_epsilon = 1e-06
MESH = pl.DeviceIdType.MESH
NORM_ROWS = 64
LANES = 128
BATCH = 4
EARLY = 2
LAG = 2
VMEM_BYTES = 64000000


class Layout:
    def __init__(self, seqs, groups):
        self.seqs = seqs
        self.groups = groups
        self.sides = 2 if seqs % 2 == 0 else 1
        self.cores = 2 if groups % 2 == 0 else 1
        self.planes = seqs // self.sides
        self.ranks = groups // self.cores
        self.per_plane = self.sides * groups
        seq = lax.axis_index("sp")
        group = lax.axis_index("tp")
        self.me = seq * groups + group
        self.seq = seq
        self.group = group
        self.side = lax.rem(seq, self.sides)
        self.plane = seq // self.sides
        self.core = lax.rem(group, self.cores)
        self.rank = group // self.cores
        self.upper = (2 * self.plane >= self.planes).astype(jnp.int32)
        self.inner = self.plane + 1 - 2 * self.upper
        self.outer = self.plane - 1 + 2 * self.upper
        self.has_outer = (self.outer >= 0) & (self.outer < self.planes)
        self.is_middle = (2 * self.inner >= self.planes) != (self.upper == 1)

    def far_plane(self, step):
        return self.upper * step + (1 - self.upper) * (self.planes - 1 - step)

    def send_seq(self, half):
        side = lax.rem(self.side + half + self.core, self.sides)
        return self.far_plane(half // self.sides) * self.sides + side

    def near_half(self):
        step = jnp.int32(0)
        if self.planes > 1:
            step = self.upper * (self.plane - 1) + (1 - self.upper) * (self.planes - 2 - self.plane)
        return step * self.sides + self.straight()

    def straight(self):
        return lax.rem(self.sides - self.core, self.sides)

    def opens(self, index):
        first = self.near_half() * self.groups
        late = index - EARLY
        late = late + EARLY * (late >= first).astype(jnp.int32)
        return (index >= EARLY) & (lax.rem(late, self.groups) == 0)

    def place(self, index):
        first = self.near_half() * self.groups
        late = index - EARLY
        late = late + EARLY * (late >= first).astype(jnp.int32)
        number = jnp.where(index < EARLY, first + index, late)
        half = number // self.groups
        turn = lax.rem(number, self.groups)
        if self.planes > 2:
            last_half = self.near_half() - self.straight() + self.sides - 1
            shift = jnp.where(self.side == 0, self.ranks - self.rank, 1)
            turned = lax.rem(turn + self.cores * shift, self.groups)
            turn = jnp.where((half == last_half) & (self.core == 0), turned, turn)
        return half, turn

    def send_group(self, turn):
        rank = lax.rem(self.rank + turn // self.cores, self.ranks)
        return rank * self.cores + lax.rem(self.core + turn, self.cores)

    def source_plane(self, step):
        near = self.planes - self.planes // 2
        plane = self.upper * (self.planes - 1 - self.plane) + (1 - self.upper) * self.plane
        first = lax.rem(plane + step, near)
        later = self.planes - 1 - (step - near)
        is_near = (step < near).astype(jnp.int32)
        plane = is_near * first + (1 - is_near) * later
        return self.upper * (self.planes - 1 - plane) + (1 - self.upper) * plane

    def source(self, index):
        within = lax.rem(index, self.per_plane)
        turn = lax.rem(within, self.groups)
        core = lax.rem(self.core + self.cores - lax.rem(turn, self.cores), self.cores)
        flip = lax.rem(within // self.groups + core, self.sides)
        side = lax.rem(self.side + self.sides - flip, self.sides)
        rank = lax.rem(self.rank + self.ranks - turn // self.cores, self.ranks)
        plane = self.source_plane(index // self.per_plane)
        return (plane * self.sides + side) * self.groups + rank * self.cores + core


def read_block(query, offsets, earlier, keys, values, head_dim):
    scores = lax.dot_general(
        query, keys, (((1,), (1,)), ((), ())), preferred_element_type=jnp.float32
    )
    scores = scores * head_dim ** (-0.5) + offsets
    soft = jnp.log1p(jnp.exp(-jnp.abs(scores)))
    rest = -jnp.maximum(scores, 0.0) - soft
    positions = scores.shape[1]
    sums = jnp.zeros((scores.shape[0], 2 * positions), jnp.float32)
    left = rest
    for _ in range(3):
        piece = left.astype(jnp.bfloat16)
        left = left - piece.astype(jnp.float32)
        sums = sums + jnp.dot(piece, earlier, preferred_element_type=jnp.float32)
    later = sums[:, :positions]
    weights = jnp.exp(jnp.minimum(scores, 0.0) - soft + later).astype(jnp.bfloat16)
    reading = jnp.dot(weights, values, preferred_element_type=jnp.float32)
    return reading, sums[:, positions:]


def later_matrix(positions):
    row = lax.broadcasted_iota(jnp.int32, (positions, 2 * positions), 0)
    col = lax.broadcasted_iota(jnp.int32, (positions, 2 * positions), 1)
    return ((row > col) | (col >= positions)).astype(jnp.float32).astype(jnp.bfloat16)


def exchange_kernel(
    seqs,
    groups,
    local_heads,
    x_hbm,
    gain_hbm,
    key_w_hbm,
    value_w_hbm,
    query_hbm,
    offset_hbm,
    arrived,
    block_read,
    block_rest,
    masked_query,
    offsets,
    x_buf,
    gain,
    query,
    offset,
    normed,
    key_w,
    value_w,
    outgoing,
    x_sem,
    w_sem,
    small_sem,
    send_sem,
    recv_sem,
    round_sem,
):
    positions = x_buf.shape[1]
    width = x_buf.shape[2]
    columns = query.shape[1]
    head_dim = columns // local_heads
    pad = masked_query.shape[0]
    devices = seqs * groups
    at = Layout(seqs, groups)
    me = at.me

    def x_copy(half):
        return pltpu.make_async_copy(x_hbm.at[at.send_seq(half)], x_buf.at[half], x_sem.at[half])

    def w_copy(turn, part):
        group = at.send_group(turn)
        cols = pl.ds(pl.multiple_of(group * columns, columns), columns)
        source = (key_w_hbm, value_w_hbm)[part].at[:, cols]
        return pltpu.make_async_copy(source, (key_w, value_w)[part].at[turn], w_sem.at[part, turn])

    small_copies = (
        pltpu.make_async_copy(gain_hbm, gain, small_sem.at[0]),
        pltpu.make_async_copy(query_hbm, query, small_sem.at[1]),
        pltpu.make_async_copy(offset_hbm, offset, small_sem.at[2]),
    )

    barrier = pltpu.get_barrier_semaphore()

    def signal(semaphore, plane, side, rank, core):
        pl.semaphore_signal(
            semaphore,
            inc=1,
            device_id=(plane * at.sides + side, rank * at.cores + core),
            device_id_type=MESH,
        )

    def signal_sides(semaphore, cores):
        for step in range(1, at.sides):
            for core in cores:
                signal(semaphore, at.plane, lax.rem(at.side + step, at.sides), at.rank, core)

    def signal_inner(semaphore):
        signal(semaphore, at.inner, at.side, at.rank, at.core)

    def signal_outer(semaphore):
        @pl.when(at.has_outer)
        def _():
            signal(semaphore, at.outer, at.side, at.rank, at.core)

    def greet():
        if at.planes > 1:

            @pl.when(at.is_middle)
            def _():
                for core in range(at.cores):
                    signal(barrier, at.inner, at.side, at.rank, core)

            @pl.when(at.has_outer)
            def _():
                for core in range(at.cores):
                    signal(barrier, at.outer, at.side, at.rank, core)

        cores = range(at.cores)
        signal_sides(barrier, cores)
        for step in range(1, at.ranks):
            for core in cores:
                signal(barrier, at.plane, at.side, lax.rem(at.rank + step, at.ranks), core)
        for step in range(1, at.cores):
            signal(barrier, at.plane, at.side, at.rank, lax.rem(at.core + step, at.cores))

    def meet():
        columns_met = at.sides + at.ranks - 1 + (at.planes > 1)
        pl.semaphore_wait(barrier, columns_met * at.cores - 1)
        signal_sides(round_sem.at[0], (at.core,))

    def pass_inwards():
        @pl.when(at.is_middle)
        def _():
            signal_inner(round_sem.at[2])

        @pl.when(jnp.logical_not(at.is_middle))
        def _():
            signal_inner(round_sem.at[1])

    def meet_plane():
        pl.semaphore_wait(round_sem.at[0], at.sides - 1)
        if at.planes > 1:
            pl.when(jnp.logical_not(at.has_outer))(pass_inwards)

    def meet_outer():
        if at.planes > 1:

            @pl.when(at.has_outer)
            def _():
                pl.semaphore_wait(round_sem.at[1], 1)
                pass_inwards()

    def meet_planes():
        if at.planes > 1:

            @pl.when(at.is_middle)
            def _():
                pl.semaphore_wait(round_sem.at[2], 1)

            @pl.when(jnp.logical_not(at.is_middle))
            def _():
                pl.semaphore_wait(round_sem.at[3], 1)

            signal_outer(round_sem.at[3])

    near = at.near_half()
    x_copy(near).start()
    small_copies[0].start()
    greet()
    w_copy(0, 0).start()
    w_copy(0, 1).start()
    x_copy(near).wait()
    small_copies[0].wait()
    for turn in range(1, groups):
        w_copy(turn, 0).start()
        w_copy(turn, 1).start()
    small_copies[1].start()
    small_copies[2].start()

    @pl.loop(0, seqs)
    def _(half):
        @pl.when(half != near)
        def _():
            x_copy(half).start()

    def block_rows(device):
        return pl.ds(pl.multiple_of(device * positions, positions), positions)

    def remote(half, turn, part):
        seq = at.send_seq(half)
        group = at.send_group(turn)
        device = seq * groups + group
        cols = pl.ds(part * columns, columns)
        return device, pltpu.make_async_remote_copy(
            src_ref=outgoing.at[half, turn, :, cols],
            dst_ref=arrived.at[block_rows(me), cols],
            send_sem=send_sem,
            recv_sem=recv_sem.at[at.plane * at.sides + lax.rem(half, at.sides)],
            device_id=(seq, group),
            device_id_type=MESH,
        )

    def launch(half, turn, part):
        device, copy = remote(half, turn, part)

        @pl.when(device != me)
        def _():
            copy.start()

        @pl.when(device == me)
        def _():
            cols = slice(part * columns, (part + 1) * columns)
            arrived[block_rows(me), cols] = outgoing[half, turn, :, cols]

    def launch_both(index):
        half, turn = at.place(index)
        launch(half, turn, 0)
        launch(half, turn, 1)

    def norm(half):
        @pl.loop(0, positions // NORM_ROWS)
        def _(chunk):
            rows = pl.ds(pl.multiple_of(chunk * NORM_ROWS, NORM_ROWS), NORM_ROWS)
            squares = jnp.zeros((NORM_ROWS, LANES), jnp.float32)
            for first in range(0, width, LANES):
                wide = x_buf[half, rows, first : first + LANES].astype(jnp.float32)
                squares = squares + wide * wide
            scale = lax.rsqrt(jnp.sum(squares, axis=-1, keepdims=True) / width + norm_epsilon)
            for first in range(0, width, LANES):
                cols = slice(first, first + LANES)
                wide = x_buf[half, rows, cols].astype(jnp.float32)
                normed[rows, cols] = (
                    wide * scale * gain[cols].astype(jnp.float32).reshape(1, LANES)
                ).astype(jnp.bfloat16)

    def project(half, turn, part):
        weight = (key_w, value_w)[part]
        outgoing[half, turn, :, part * columns : (part + 1) * columns] = jnp.dot(
            normed[...], weight[turn], preferred_element_type=jnp.float32
        ).astype(jnp.bfloat16)

    stages = (meet_plane, meet_outer, meet_planes)

    @pl.loop(0, devices)
    def _(index):
        half, turn = at.place(index)
        opens = at.opens(index)

        @pl.when(opens & (half != near))
        def _():
            x_copy(half).wait()

        @pl.when(opens | (index == 0) | (index == EARLY) | ((half == near) & (turn == EARLY)))
        def _():
            norm(half)

        fresh = (index < EARLY) | ((index < EARLY + groups) & (turn >= EARLY))

        @pl.when(fresh)
        def _():
            w_copy(turn, 0).wait()

        project(half, turn, 0)

        @pl.when(index == 0)
        def _():
            meet()
            launch(half, turn, 0)

        @pl.when((index > 0) & (index <= EARLY))
        def _():
            early_half, early_turn = at.place(index - 1)
            launch(early_half, early_turn, 1)

        @pl.when(fresh)
        def _():
            w_copy(turn, 1).wait()

        project(half, turn, 1)

        for number, stage in enumerate(stages):

            @pl.when(index == 2 + number)
            def _():
                stage()

        @pl.when((index > 0) & (index < EARLY))
        def _():
            launch(half, turn, 0)

        @pl.when(index == EARLY + LAG)
        def _():
            @pl.loop(EARLY, EARLY + LAG)
            def _(number):
                launch_both(number)

        @pl.when(index > EARLY + LAG)
        def _():
            launch_both(index - 1)

    small_copies[1].wait()
    small_copies[2].wait()
    row = lax.broadcasted_iota(jnp.int32, (pad, columns), 0)
    col = lax.broadcasted_iota(jnp.int32, (pad, columns), 1)
    masked_query[...] = jnp.where(
        row == col // head_dim,
        jnp.broadcast_to(query[...].astype(jnp.float32), (pad, columns)),
        0.0,
    ).astype(jnp.bfloat16)
    score_row = lax.broadcasted_iota(jnp.int32, (pad, positions), 0)
    head_offsets = jnp.zeros((pad, positions), jnp.float32)
    for head in range(local_heads):
        head_offsets = jnp.where(
            score_row == head, offset[at.group * local_heads + head], head_offsets
        )
    offsets[...] = head_offsets
    launch_both(jnp.int32(devices - 1))

    earlier = later_matrix(positions)

    def wait_group(number):
        plane = at.source_plane(number // at.sides)
        half = lax.rem(number, at.sides)
        semaphore = recv_sem.at[plane * at.sides + half]

        def wait_blocks(count):
            whole = arrived.at[pl.ds(0, count * positions)]
            pltpu.make_async_copy(whole, whole, semaphore).wait()

        with_own = (plane == at.plane) & (half == at.straight())

        @pl.when(with_own)
        def _():
            wait_blocks(groups - 1)

        @pl.when(jnp.logical_not(with_own))
        def _():
            wait_blocks(groups)

    @pl.loop(0, seqs - 1)
    def _(number):
        wait_group(number)

        @pl.loop(0, groups // BATCH)
        def _(batch):
            for k in range(BATCH):
                source = at.source(number * groups + batch * BATCH + k)
                rows = block_rows(source)
                reading, rest = read_block(
                    masked_query[...],
                    offsets[...],
                    earlier,
                    arrived[rows, :columns],
                    arrived[rows, columns:],
                    head_dim,
                )
                block_read[source] = reading
                block_rest[source] = rest

    sent = arrived.at[pl.ds(0, (devices - 1) * positions)]
    pltpu.make_async_copy(sent, sent, send_sem).wait()
    wait_group(jnp.int32(seqs - 1))


def finish_kernel(
    seqs,
    groups,
    local_heads,
    arrived,
    block_read,
    block_rest,
    masked_query,
    offsets,
    keys_hbm,
    values_hbm,
    read_hbm,
    last_read,
    last_rest,
    read,
    out_sem,
    read_sem,
):
    devices = seqs * groups
    length = arrived.shape[0]
    positions = length // devices
    columns = masked_query.shape[1]
    head_dim = columns // local_heads
    at = Layout(seqs, groups)
    pieces = out_sem.shape[1]
    span = length // pieces

    def out_copies(piece):
        rows = pl.ds(pl.multiple_of(piece * span, span), span)
        return (
            pltpu.make_async_copy(
                arrived.at[rows, pl.ds(0, columns)], keys_hbm.at[rows], out_sem.at[0, piece]
            ),
            pltpu.make_async_copy(
                arrived.at[rows, pl.ds(columns, columns)], values_hbm.at[rows], out_sem.at[1, piece]
            ),
        )

    @pl.loop(0, pieces)
    def _(piece):
        for copy in out_copies(piece):
            copy.start()

    sources = [at.source(jnp.int32(devices - groups + k)) for k in range(groups)]
    earlier = later_matrix(positions)
    last_read[...] = block_read[...]
    last_rest[...] = block_rest[...]
    for source in sources:
        rows = pl.ds(pl.multiple_of(source * positions, positions), positions)
        reading, rest = read_block(
            masked_query[...],
            offsets[...],
            earlier,
            arrived[rows, :columns],
            arrived[rows, columns:],
            head_dim,
        )
        last_read[source] = reading
        last_rest[source] = rest

    reading = jnp.zeros(last_read.shape[1:], jnp.float32)
    after = jnp.zeros(last_rest.shape[1:], jnp.float32)
    for device in reversed(range(devices)):
        scale = jnp.exp(after)
        reading = reading + jnp.concatenate([scale] * (columns // positions), axis=1) * last_read[device]
        after = after + last_rest[device]
    for head in range(local_heads):
        own_cols = slice(head * head_dim, (head + 1) * head_dim)
        part = reading[head : head + 1, own_cols]
        read[:, own_cols] = part * lax.rsqrt(
            jnp.mean(part * part, axis=-1, keepdims=True) + norm_epsilon
        )
    read_copy = pltpu.make_async_copy(read, read_hbm, read_sem)
    read_copy.start(priority=1)
    @pl.loop(0, pieces)
    def _(piece):
        for copy in out_copies(piece):
            copy.wait()

    read_copy.wait()


def shards(seqs, groups, layer_input, norm_gain, key_weight, value_weight, new_query, score_offset):
    seq_count, positions, width = layer_input.shape
    columns = new_query.shape[1]
    local_heads = score_offset.shape[0] // groups
    pad = -(-local_heads // 8) * 8
    devices = seqs * groups
    length = devices * positions
    hbm = pl.BlockSpec(memory_space=pltpu.HBM)
    vmem = pl.BlockSpec(memory_space=pltpu.VMEM)
    passed_bytes = 4 * length * columns + 4 * devices * pad * (columns + positions)
    passed = pl.pallas_call(
        functools.partial(exchange_kernel, seqs, groups, local_heads),
        out_shape=(
            pltpu.VMEM((length, 2 * columns), jnp.bfloat16),
            pltpu.VMEM((devices, pad, columns), jnp.float32),
            pltpu.VMEM((devices, pad, positions), jnp.float32),
            pltpu.VMEM((pad, columns), jnp.bfloat16),
            pltpu.VMEM((pad, positions), jnp.float32),
        ),
        in_specs=[hbm] * 6,
        out_specs=(vmem,) * 5,
        scratch_shapes=[
            pltpu.VMEM((seq_count, positions, width), jnp.bfloat16),
            pltpu.VMEM((width,), jnp.bfloat16),
            pltpu.VMEM((1, columns), jnp.bfloat16),
            pltpu.SMEM(score_offset.shape, jnp.float32),
            pltpu.VMEM((positions, width), jnp.bfloat16),
            pltpu.VMEM((groups, width, columns), jnp.bfloat16),
            pltpu.VMEM((groups, width, columns), jnp.bfloat16),
            pltpu.VMEM((seqs, groups, positions, 2 * columns), jnp.bfloat16),
            pltpu.SemaphoreType.DMA((seq_count,)),
            pltpu.SemaphoreType.DMA((2, groups)),
            pltpu.SemaphoreType.DMA((3,)),
            pltpu.SemaphoreType.DMA,
            pltpu.SemaphoreType.DMA((seqs,)),
            pltpu.SemaphoreType.REGULAR((4,)),
        ],
        compiler_params=pltpu.CompilerParams(
            collective_id=0, has_side_effects=True, vmem_limit_bytes=VMEM_BYTES - passed_bytes
        ),
    )(layer_input, norm_gain, key_weight, value_weight, new_query, score_offset)
    keys, values, read = pl.pallas_call(
        functools.partial(finish_kernel, seqs, groups, local_heads),
        out_shape=(
            jax.ShapeDtypeStruct((length, columns), jnp.bfloat16),
            jax.ShapeDtypeStruct((length, columns), jnp.bfloat16),
            jax.ShapeDtypeStruct((1, columns), jnp.float32),
        ),
        in_specs=[vmem] * 5,
        out_specs=(hbm,) * 3,
        scratch_shapes=[
            pltpu.VMEM((devices, pad, columns), jnp.float32),
            pltpu.VMEM((devices, pad, positions), jnp.float32),
            pltpu.VMEM((1, columns), jnp.float32),
            pltpu.SemaphoreType.DMA((2, 4)),
            pltpu.SemaphoreType.DMA,
        ],
        compiler_params=pltpu.CompilerParams(vmem_limit_bytes=20000000),
    )(*passed)
    return (keys[None], values[None], read)


def solution(mesh):
    seqs = mesh.shape["sp"]
    groups = mesh.shape["tp"]
    placed = (P(None, ("sp", "tp"), None), P(), P(), P(), P("sp", "tp"), P())
    return jax.shard_map(
        functools.partial(shards, seqs, groups),
        mesh=mesh,
        in_specs=placed,
        out_specs=(P("sp", None, "tp"), P("sp", None, "tp"), P("sp", "tp")),
        check_vma=False,
    )
```
